512 devices in a mesh: sp: 64 (over z, y), tp: 8 (over x, core).
Axes of the slice: x: 4, y: 8, z: 8, core: 2. Of those that a mesh axis runs over, the one named last changes fastest.
Arguments:
- resid: bfloat16 [8192, 2048], P('sp', 'tp'), may hold values from -6 to 6
- qa_nope: bfloat16 [8192, 1024], P('sp', 'tp'), may hold values from -6 to 6
- qb_nope: bfloat16 [8192, 1024], P('sp', 'tp'), may hold values from -6 to 6
- qa_rope: bfloat16 [8192, 512], P('sp', 'tp'), may hold values from -360 to 360
- qb_rope: bfloat16 [8192, 256], P('sp', 'tp'), may hold values from -360 to 360
- latent: bfloat16 [8192, 256], P('sp'), may hold values from -6 to 6
- key_rope: bfloat16 [8192, 32], P('sp'), may hold values from -4 to 4
- lat_gain: float32 [256], replicated, may hold values from 0.1 to 1.9
- wa_key: bfloat16 [256, 1024], P(None, 'tp'), may hold values from -0.375 to 0.375
- wa_val: bfloat16 [256, 1024], P(None, 'tp'), may hold values from -0.75 to 0.75
- wb_key: bfloat16 [256, 1024], P(None, 'tp'), may hold values from -0.375 to 0.375
- wb_val: bfloat16 [256, 1024], P(None, 'tp'), may hold values from -0.75 to 0.75
- gain_a: float32 [1024], P('tp'), may hold values from 0.1 to 1.9
- gain_b: float32 [1024], P('tp'), may hold values from 0.1 to 1.9
- wa_out: bfloat16 [1024, 2048], P('tp'), may hold values from -0.125 to 0.125
- wb_out: bfloat16 [1024, 2048], P('tp'), may hold values from -0.125 to 0.125
- norm1_gain: float32 [2048], replicated, may hold values from 0.1 to 1.9
- ffn_gate: bfloat16 [2048, 5632], P('sp', 'tp'), may hold values from -0.125 to 0.125
- ffn_val: bfloat16 [2048, 5632], P('sp', 'tp'), may hold values from -0.125 to 0.125
- conv_gate: float32 [3, 5632], P(None, 'tp'), may hold values from -3 to 3
- conv_val: float32 [3, 5632], P(None, 'tp'), may hold values from -3 to 3
- ffn_down: bfloat16 [5632, 2048], P('tp'), may hold values from -0.078125 to 0.078125
- norm2_gain: float32 [2048], P('tp'), may hold values from 0.1 to 1.9
Outputs:
- layer_out: bfloat16 [8192, 2048], P('sp', 'tp')
The draws below stay inside these ranges and needn't reach their ends.
All inputs are finite; a program needn't handle non-finite values.
Results may differ from the reference program's by a relative error of at most 0.017.
Values may be sent and summed in bfloat16 or wider, within the bound.
A program may use at most 128 MiB of HBM per device.

```python
import math
import jax
import jax.numpy as jnp
from jax import lax

D = 2048
HA = 16
DA = 64
HB = 8
DB = 128
DR = 32
LAT = 256
FF = 5632
KC = 3
TOKENS = 8192


def drawn(key):
    base = jnp.clip(jax.random.normal(jax.random.fold_in(key, 101), (TOKENS, DR), jnp.float32), -4.0, 4.0)
    return base


def draw_key_rope(key, part):
    base = drawn(key)
    return base.astype(jnp.bfloat16)


def draw_qa_rope(key, part):
    noise = jnp.clip(jax.random.normal(jax.random.fold_in(key, 104), (TOKENS, HA * DR), jnp.float32), -6.0, 6.0)
    return noise.astype(jnp.bfloat16)


def draw_qb_rope(key, part):
    noise = jnp.clip(jax.random.normal(jax.random.fold_in(key, 105), (TOKENS, HB * DR), jnp.float32), -6.0, 6.0)
    return noise.astype(jnp.bfloat16)


def rising_value(key, heads, width):
    noise = jnp.clip(jax.random.normal(key, (LAT, heads * width), jnp.float32), -6.0, 6.0) * LAT ** (-0.5)
    head_index = (jnp.arange(heads * width) // width).astype(jnp.float32)
    factor = 0.5 * 4.0 ** (head_index / (heads - 1))
    return (noise * factor[None, :]).astype(jnp.bfloat16)


def draw_wa_val(key, part):
    return rising_value(jax.random.fold_in(key, 201), HA, DA)


def draw_wb_val(key, part):
    return rising_value(jax.random.fold_in(key, 202), HB, DB)


def levels(stream_key, extent, shards, least, top_value):
    loudness = 1.0
    for dim, shards_of in shards:
        draws = jax.random.uniform(jax.random.fold_in(jax.random.fold_in(stream_key, 6), dim), (shards_of,), jnp.float32, least / len(shards), top_value / len(shards))
        loudness = loudness * jnp.repeat(jnp.exp(draws), extent[dim] // shards_of).reshape((-1,) + (1,) * (len(extent) - 1 - dim))
    return loudness


def gaussian(key, shape, scale, bound, cuts=(), kind=jnp.bfloat16):
    result = scale * jax.random.normal(key, shape, jnp.float32)
    if cuts:
        result = result * levels(key, shape, cuts, -0.22, 0.18)
    return jnp.clip(result, -bound, bound).astype(kind)


def setup_inputs(seed: int = 0) -> dict:
    key_list = jax.random.split(jax.random.key(seed), 24)
    resid = gaussian(key_list[0], (TOKENS, D), 1.0, 6.0, ((0, 64), (1, 8)))
    qa_nope = gaussian(key_list[1], (TOKENS, HA * DA), 1.0, 6.0, ((0, 64), (1, 8)))
    qb_nope = gaussian(key_list[2], (TOKENS, HB * DB), 1.0, 6.0, ((0, 64), (1, 8)))
    qa_rope = draw_qa_rope(jax.random.fold_in(key_list[23], 71), 0)
    qb_rope = draw_qb_rope(jax.random.fold_in(key_list[23], 71), 0)
    latent = gaussian(key_list[5], (TOKENS, LAT), 1.0, 6.0, ((0, 64),))
    key_rope = draw_key_rope(jax.random.fold_in(key_list[23], 71), 0)
    lat_gain = jnp.clip(1.0 + 0.18 * jax.random.normal(key_list[7], (LAT,), jnp.float32), 0.1, 1.9)
    wa_key = gaussian(key_list[8], (LAT, HA * DA), LAT ** -0.5, 0.375, ((1, 8),))
    wa_val = draw_wa_val(jax.random.fold_in(key_list[23], 71), 0)
    wb_key = gaussian(key_list[10], (LAT, HB * DB), LAT ** -0.5, 0.375, ((1, 8),))
    wb_val = draw_wb_val(jax.random.fold_in(key_list[23], 71), 0)
    gain_a = jnp.clip(1.0 + 0.18 * jax.random.normal(key_list[12], (HA * DA,), jnp.float32), 0.1, 1.9)
    gain_b = jnp.clip(1.0 + 0.18 * jax.random.normal(key_list[13], (HB * DB,), jnp.float32), 0.1, 1.9)
    wa_out = gaussian(key_list[14], (HA * DA, D), (HA * DA + HB * DB) ** -0.5, 0.125, ((0, 8),))
    wb_out = gaussian(key_list[15], (HB * DB, D), (HA * DA + HB * DB) ** -0.5, 0.125, ((0, 8),))
    norm1_gain = jnp.clip(1.0 + 0.18 * jax.random.normal(key_list[16], (D,), jnp.float32), 0.1, 1.9)
    ffn_gate = gaussian(key_list[17], (D, FF), D ** -0.5, 0.125, ((0, 64), (1, 8)))
    ffn_val = gaussian(key_list[18], (D, FF), D ** -0.5, 0.125, ((0, 64), (1, 8)))
    conv_gate = gaussian(key_list[19], (KC, FF), 0.577, 3.0, ((1, 8),), jnp.float32)
    conv_val = gaussian(key_list[20], (KC, FF), 0.577, 3.0, ((1, 8),), jnp.float32)
    ffn_down = gaussian(key_list[21], (FF, D), FF ** -0.5, 0.078125, ((0, 8),))
    norm2_gain = jnp.clip(1.0 + 0.18 * jax.random.normal(key_list[22], (D,), jnp.float32), 0.1, 1.9)
    return dict(resid=resid, qa_nope=qa_nope, qb_nope=qb_nope, qa_rope=qa_rope, qb_rope=qb_rope, latent=latent, key_rope=key_rope, lat_gain=lat_gain, wa_key=wa_key, wa_val=wa_val, wb_key=wb_key, wb_val=wb_val, gain_a=gain_a, gain_b=gain_b, wa_out=wa_out, wb_out=wb_out, norm1_gain=norm1_gain, ffn_gate=ffn_gate, ffn_val=ffn_val, conv_gate=conv_gate, conv_val=conv_val, ffn_down=ffn_down, norm2_gain=norm2_gain)


THETA = 10000.0
EPS_RMS = 1e-06
EPS_NORM = 1e-05
ALPHA = 2.0 ** 0.25

def stored(values):
    return lax.optimization_barrier(values.astype(jnp.bfloat16))

def rotary(values, positions):
    half = values.shape[-1] // 2
    freq = THETA ** (-jnp.arange(half, dtype=jnp.float32) * 2.0 / values.shape[-1])
    angle = positions.astype(jnp.float32)[:, None] * freq[None, :]
    if values.ndim == 3:
        angle = angle[:, None, :]
    cosine = jnp.cos(angle)
    sine = jnp.sin(angle)
    first = values[..., :half]
    second = values[..., half:]
    return jnp.concatenate([first * cosine - second * sine, second * cosine + first * sine], axis=-1)

def rms_scale(values, gain):
    wide = values.astype(jnp.float32)
    return wide * lax.rsqrt(lax.optimization_barrier(jnp.mean(wide * wide, axis=-1, keepdims=True)) + EPS_RMS) * gain.astype(jnp.float32)

def layer_norm(values, gain):
    center = lax.optimization_barrier(jnp.mean(values, axis=-1, keepdims=True))
    shifted = values - center
    spread = lax.optimization_barrier(jnp.mean(shifted * shifted, axis=-1, keepdims=True))
    return shifted * lax.rsqrt(spread + EPS_NORM) * gain.astype(jnp.float32)

def attend(query, q_rot, keys, k_rot, vals):
    total_rows, heads, width = query.shape
    scale = (width + k_rot.shape[-1]) ** (-0.5)
    block = math.gcd(512, total_rows)
    key_pos = jnp.arange(total_rows)
    keys_wide = keys.astype(jnp.float32)
    rot_wide = k_rot.astype(jnp.float32)
    vals_wide = vals.astype(jnp.float32)

    def one_block(index):
        start = index * block
        q_part = lax.dynamic_slice_in_dim(query, start, block, 0).astype(jnp.float32)
        r_part = lax.dynamic_slice_in_dim(q_rot, start, block, 0).astype(jnp.float32)
        scores = jnp.einsum('qhd,khd->hqk', q_part, keys_wide) + jnp.einsum('qhr,kr->hqk', r_part, rot_wide)
        scores = scores * scale
        q_pos = start + jnp.arange(block)
        allowed = key_pos[None, :] <= q_pos[:, None]
        scores = jnp.where(allowed[None], scores, -jnp.inf)
        top = lax.optimization_barrier(jnp.max(scores, axis=-1, keepdims=True))
        weights = jnp.exp(scores - top)
        total = lax.optimization_barrier(jnp.sum(weights, axis=-1))
        rounded = stored(weights).astype(jnp.float32)
        mixed = jnp.einsum('hqk,khd->qhd', rounded, vals_wide)
        return mixed / jnp.transpose(total)[:, :, None]
    out = lax.map(one_block, jnp.arange(total_rows // block)).reshape(total_rows, heads * width)
    return out

def causal_conv(values, taps):
    count = values.shape[0]
    padded = jnp.pad(values.astype(jnp.float32), ((KC - 1, 0), (0, 0)))
    total = jnp.zeros(values.shape, jnp.float32)
    for tap in range(KC):
        total = total + taps[tap].astype(jnp.float32) * padded[tap:tap + count]
    return total

def reference(resid, qa_nope, qb_nope, qa_rope, qb_rope, latent, key_rope, lat_gain, wa_key, wa_val, wb_key, wb_val, gain_a, gain_b, wa_out, wb_out, norm1_gain, ffn_gate, ffn_val, conv_gate, conv_val, ffn_down, norm2_gain):
    positions = jnp.arange(TOKENS)
    lat_n = stored(rms_scale(latent, lat_gain))
    k_rot = stored(rotary(key_rope.astype(jnp.float32), positions))

    def group(q_nope, q_rope, w_key, w_val, width):
        heads = q_nope.shape[1] // width
        q_rot = stored(rotary(q_rope.astype(jnp.float32).reshape(TOKENS, heads, DR), positions))
        keys = stored(jnp.dot(lat_n, w_key, preferred_element_type=jnp.float32)).reshape(TOKENS, heads, width)
        vals = stored(jnp.dot(lat_n, w_val, preferred_element_type=jnp.float32)).reshape(TOKENS, heads, width)
        return attend(q_nope.reshape(TOKENS, heads, width), q_rot, keys, k_rot, vals)
    raw_a = group(qa_nope, qa_rope, wa_key, wa_val, DA)
    raw_b = group(qb_nope, qb_rope, wb_key, wb_val, DB)
    energy = lax.optimization_barrier(jnp.sum(raw_a * raw_a, axis=-1)) + lax.optimization_barrier(jnp.sum(raw_b * raw_b, axis=-1))
    factor = lax.rsqrt(energy / (HA * DA + HB * DB) + EPS_RMS)[:, None]
    part_a = stored(raw_a * factor * gain_a.astype(jnp.float32))
    part_b = stored(raw_b * factor * gain_b.astype(jnp.float32))
    mix = jnp.dot(part_a, wa_out, preferred_element_type=jnp.float32) + jnp.dot(part_b, wb_out, preferred_element_type=jnp.float32)
    first = stored(layer_norm(ALPHA * resid.astype(jnp.float32) + mix, norm1_gain))
    gate_up = stored(jnp.dot(first, ffn_gate, preferred_element_type=jnp.float32))
    val_up = stored(jnp.dot(first, ffn_val, preferred_element_type=jnp.float32))
    gate_c = causal_conv(gate_up, conv_gate)
    val_c = causal_conv(val_up, conv_val)
    hidden = stored(jax.nn.silu(gate_c) * val_c)
    down = jnp.dot(hidden, ffn_down, preferred_element_type=jnp.float32)
    return layer_norm(ALPHA * first.astype(jnp.float32) + down, norm2_gain).astype(jnp.bfloat16)
```

```python
import jax
import jax.numpy as jnp
from jax import lax
from jax.experimental import pallas as pl
from jax.experimental.pallas import tpu as pltpu
from jax.sharding import PartitionSpec as P

D = 2048
HA = 16
DA = 64
HB = 8
DB = 128
DR = 32
LAT = 256
KC = 3
ROWS = 128
COLS = 256
UNITS = 704
MAIN = 640
HALO = 16
N = 8

THETA = 10000.0
EPS_RMS = 1e-06
EPS_NORM = 1e-05
ALPHA = 2.0**0.25
LOG2E = 1.4426950408889634
LOW = -1e30
MESH = pl.DeviceIdType.MESH
F32 = jnp.float32
BF16 = jnp.bfloat16


def dot(a, b):
    return jnp.dot(a, b, preferred_element_type=F32)


def dot_t(a, b):
    return lax.dot_general(a, b, (((1,), (1,)), ((), ())), preferred_element_type=F32)


def wrap(v):
    return lax.rem(v, N)


def kernel(
    cosine,
    sine,
    resid,
    qa_nope,
    qb_nope,
    qa_rope,
    qb_rope,
    latent,
    key_rope,
    lat_gain,
    wa_key,
    wa_val,
    wb_key,
    wb_val,
    gain_a,
    gain_b,
    wa_out,
    wb_out,
    norm1_gain,
    ffn_gate,
    ffn_val,
    conv_gate,
    conv_val,
    ffn_down,
    norm2_gain,
    out,
    lat,
    wgt,
    q_lat,
    q_rot,
    acc,
    top,
    total,
    w_out,
    w_down,
    mix_out,
    mix_in,
    energy,
    pre,
    first,
    first_own,
    up,
    hidden,
    down_out,
    down_in,
    stats,
    local_sem,
    l1s,
    l1r,
    w1s,
    w1r,
    l2s,
    l2r,
    dds,
    ddr,
    w2s,
    w2r,
    mxs,
    mxr,
    ens,
    enr,
    prs,
    prr,
    hls,
    hlr,
    dns,
    dnr,
    sts,
    srr,
):
    sp = lax.axis_index("sp")
    tp = lax.axis_index("tp")
    core = lax.rem(tp, 2)
    z = lax.div(sp, N)
    y = lax.rem(sp, N)
    alpha = y + core * (z - y)
    beta = z + core * (y - z)
    sa = 1 + 7 * core
    sb = 8 - 7 * core
    partner = (sp, tp + 1 - 2 * core)
    nxt = (lax.rem(sp + 1, N * N), tp)
    prv = (lax.rem(sp + N * N - 1, N * N), tp)

    def along_a(k):
        return (wrap(alpha + k) * sa + beta * sb, tp)

    def along_b(k):
        return (alpha * sa + wrap(beta + k) * sb, tp)

    def along_tp(k):
        return (sp, wrap(tp + k))

    def remote(src, dst, send, recv, device):
        return pltpu.make_async_remote_copy(
            src_ref=src, dst_ref=dst, send_sem=send, recv_sem=recv, device_id=device, device_id_type=MESH
        )

    pending = []

    def send(src, dst, ssem, rsem, device):
        copy = remote(src, dst, ssem, rsem, device)
        copy.start()
        pending.append(copy)

    def arrived(ref, rsem):
        remote(ref, ref, l1s.at[0], rsem, partner).wait_recv()

    barrier = pltpu.get_barrier_semaphore()
    peers = [along_a(k) for k in range(1, N)] + [along_b(1), along_b(N - 1)]
    peers += [along_tp(k) for k in range(1, N)] + [nxt, prv]
    for device in peers:
        pl.semaphore_signal(barrier, inc=1, device_id=device, device_id_type=MESH)

    local = [
        pltpu.make_async_copy(wa_out, w_out.at[0:128], local_sem.at[0]),
        pltpu.make_async_copy(wb_out, w_out.at[128:256], local_sem.at[1]),
        pltpu.make_async_copy(ffn_down, w_down, local_sem.at[2]),
    ]
    for copy in local:
        copy.start()

    half = pl.ds(pl.multiple_of(core * 64, 64), 64)
    wide = latent[half, :].astype(F32)
    wide = wide * lax.rsqrt(jnp.mean(wide * wide, axis=1, keepdims=True) + EPS_RMS) * lat_gain[...]
    lat_n = wide.astype(BF16)

    def rotated(v, c, s):
        return v * c + jnp.concatenate([v[:, DR // 2 :], v[:, : DR // 2]], axis=1) * s

    k_rot = rotated(key_rope[half, :].astype(F32), cosine[half, :], sine[half, :])
    k_wide = jnp.concatenate([k_rot, jnp.zeros((64, 128 - DR), F32)], axis=1)
    k_wide = jnp.concatenate([k_wide, jnp.zeros((64, 128), F32)], axis=0)
    k_t = k_wide.T
    k_packed = jnp.concatenate([k_t[0:16, 0:64], k_t[16:32, 0:64]], axis=1)
    lat[core, beta, alpha, 0:64, :] = lat_n[:, :128]
    lat[core, beta, alpha, 64:128, :] = lat_n[:, 128:]
    lat[core, beta, alpha, 128:144, :] = k_packed.astype(BF16)
    wgt[beta, alpha, :, 0:MAIN] = ffn_gate[:, :MAIN]
    wgt[beta, alpha, :, MAIN : 2 * MAIN] = ffn_val[:, :MAIN]
    wgt[beta, alpha, :, 2 * MAIN :] = jnp.concatenate(
        [ffn_gate[:, MAIN:].astype(F32), ffn_val[:, MAIN:].astype(F32)], axis=1
    ).astype(BF16)

    pl.semaphore_wait(barrier, len(peers))

    mine = lat.at[core, beta, alpha]
    for k in (4, 3, 5, 2, 6, 1, 7):
        send(mine, mine, l1s.at[k - 1], l1r.at[alpha], along_a(k))

    def weight_step(step, forward, backward):
        if forward:
            block = wgt.at[beta, wrap(alpha + N - step)]
            if step:
                arrived(block, w1r.at[wrap(alpha + N - step)])
            send(block, block, w1s.at[step], w1r.at[wrap(alpha + N - step)], along_a(1))
        if backward:
            block = wgt.at[beta, wrap(alpha + step)]
            if step:
                arrived(block, w1r.at[wrap(alpha + step)])
            send(block, block, w1s.at[4 + step], w1r.at[wrap(alpha + step)], along_a(N - 1))

    weight_step(0, True, True)

    q_scale_a = (DA + DR) ** (-0.5) * LOG2E
    q_scale_b = (DB + DR) ** (-0.5) * LOG2E
    for h in range(2):
        part = dot_t(qa_nope[:, h * DA : (h + 1) * DA], wa_key[:, h * DA : (h + 1) * DA])
        q_lat[h * ROWS : (h + 1) * ROWS, :] = (part * q_scale_a).astype(BF16)
        turned = rotated(qa_rope[:, h * DR : (h + 1) * DR].astype(F32), cosine[...], sine[...])
        q_rot[h * ROWS : (h + 1) * ROWS, :] = (turned * q_scale_a).astype(BF16)
    part = dot_t(qb_nope[...], wb_key[...])
    q_lat[2 * ROWS :, :] = (part * q_scale_b).astype(BF16)
    turned = rotated(qb_rope[...].astype(F32), cosine[...], sine[...])
    q_rot[2 * ROWS :, :] = (turned * q_scale_b).astype(BF16)
    acc[...] = jnp.zeros_like(acc)
    top[...] = jnp.full_like(top, LOW)
    total[...] = jnp.zeros_like(total)

    def lat_piece(b, p):
        return lat.at[core, b, pl.ds(4 * p, 4)]

    def lat_pass(d, p, forward, backward):
        for go, b, k, base in (
            (forward, wrap(beta + N - d), 1, 0),
            (backward, wrap(beta + d), N - 1, 7),
        ):
            if go:
                if d:
                    arrived(lat_piece(b, p), l2r.at[2 * b + p])
                at = base + (2 * d + p if d < 3 else 6)
                send(lat_piece(b, p), lat_piece(b, p), l2s.at[at], l2r.at[2 * b + p], along_b(k))

    def hand_over(b):
        send(lat.at[core, b], lat.at[core, b], dds.at[b], ddr.at[b], partner)

    def wgt_piece(b, p):
        return wgt.at[b, pl.ds(2 * p, 2)]

    def wgt_pass(d, p, forward=True, backward=True):
        for go, b, k, base in (
            (forward, wrap(beta + N - d), 1, 0),
            (backward, wrap(beta + d), N - 1, 14),
        ):
            if go:
                if d:
                    arrived(wgt_piece(b, p), w2r.at[4 * b + p])
                at = base + 4 * d + (p if d < 3 or k == 1 else p - 2)
                send(wgt_piece(b, p), wgt_piece(b, p), w2s.at[at], w2r.at[4 * b + p], along_b(k))

    for k in range(1, N):
        block = lat.at[core, beta, wrap(alpha + k)]
        arrived(block, l1r.at[wrap(alpha + k)])
    lat_pass(0, 0, True, True)
    lat_pass(0, 1, True, True)
    hand_over(beta)
    weight_step(1, True, True)
    weight_step(2, True, True)
    lat_pass(1, 0, True, True)
    weight_step(3, True, False)
    lat_pass(1, 1, True, True)
    hand_over(wrap(beta + N - 1))
    hand_over(wrap(beta + 1))
    lat_pass(2, 0, True, True)
    for k in (3, 4):
        a = wrap(alpha + k)
        arrived(wgt.at[beta, a], w1r.at[a])
    wgt_pass(0, 0)
    lat_pass(2, 1, True, True)
    hand_over(wrap(beta + N - 2))
    hand_over(wrap(beta + 2))
    wgt_pass(0, 1)
    lat_pass(3, 0, True, False)
    lat_pass(3, 1, False, True)
    wgt_pass(0, 2)
    wgt_pass(0, 3)
    for b, p in ((wrap(beta + N - 3), 1), (wrap(beta + 3), 0)):
        arrived(lat_piece(b, p), l2r.at[2 * b + p])
    hand_over(wrap(beta + N - 3))
    hand_over(wrap(beta + 3))
    b = wrap(beta + 4)
    arrived(lat_piece(b, 0), l2r.at[2 * b])
    arrived(lat_piece(b, 1), l2r.at[2 * b + 1])
    hand_over(b)

    def offset(i):
        steps = lax.div(i + 1, 2)
        return wrap(N + steps * (1 - 2 * lax.rem(i, 2)))

    def attend(i):
        b0 = wrap(z + offset(i))
        b1 = wrap(y + offset(i))
        theirs = b1 + core * (b0 - b1)
        arrived(lat.at[1 - core, theirs], ddr.at[theirs])
        left, right, roped = [], [], []
        for half_of, b in ((0, b0), (1, b1)):
            left.append(lat[half_of, b, :, 0:64, :].reshape(512, 128))
            right.append(lat[half_of, b, :, 64:128, :].reshape(512, 128))
            x = lat[half_of, b, :, 128:144, :]
            upper = [jnp.concatenate([x[a][:, :64], x[a + 1][:, :64]], axis=1) for a in range(0, N, 2)]
            lower = [jnp.concatenate([x[a][:, 64:], x[a + 1][:, 64:]], axis=1) for a in range(0, N, 2)]
            roped.append(
                jnp.concatenate(
                    [jnp.concatenate(upper, axis=1), jnp.concatenate(lower, axis=1)], axis=0
                )
            )
        keys = jnp.concatenate(
            [jnp.concatenate(left, axis=0), jnp.concatenate(right, axis=0)], axis=1
        )
        ropes = jnp.concatenate(roped, axis=1)
        scores = dot_t(q_lat[...], keys) + dot(q_rot[...], ropes)
        j = lax.broadcasted_iota(jnp.int32, (1, 1024), 1)
        a = lax.shift_right_logical(lax.bitwise_and(j, 511), 6)
        r = lax.bitwise_and(j, 63)
        spots = jnp.where(j < 512, b0 * 1024 + a * 128 + r, a * 1024 + b1 * 128 + 64 + r)
        rows = lax.broadcasted_iota(jnp.int32, (3 * ROWS, 1), 0)
        rows = sp * ROWS + lax.bitwise_and(rows, ROWS - 1)
        scores = jnp.where(spots <= rows, scores, LOW)
        old = top[:, 0:1]
        new = jnp.maximum(old, jnp.max(scores, axis=1, keepdims=True))
        weights = jnp.exp2(scores - new)
        shrink = jnp.exp2(old - new)
        total[...] = total[...] * shrink + jnp.sum(weights, axis=1, keepdims=True)
        acc[...] = acc[...] * shrink + dot(weights.astype(BF16), keys)
        top[...] = jnp.broadcast_to(new, top.shape)

    def attend_two(e):
        def body(i, carry):
            attend(i)
            return carry

        lax.fori_loop(2 * e, 2 * e + 2, body, 0)

    for e in range(4):
        attend_two(e)
        wgt_pass(1, e)

    normed = (acc[...] / total[:, 0:1]).astype(BF16)
    raw_a = jnp.concatenate(
        [dot(normed[h * ROWS : (h + 1) * ROWS], wa_val[:, h * DA : (h + 1) * DA]) for h in range(2)], axis=1
    )
    raw_b = dot(normed[2 * ROWS :], wb_val[...])
    power = jnp.sum(raw_a * raw_a, axis=1, keepdims=True) + jnp.sum(raw_b * raw_b, axis=1, keepdims=True)
    energy[tp] = jnp.broadcast_to(power, (ROWS, ROWS)).T[0:8]
    gained = jnp.concatenate([raw_a * gain_a[...], raw_b * gain_b[...]], axis=1).astype(BF16)
    local[0].wait()
    local[1].wait()

    def of_tp(t):
        return pl.ds(pl.multiple_of(t * COLS, COLS), COLS)

    order = (4, 5, 3, 2, 6, 7, 1)
    for k in order:
        t = wrap(tp + k)
        mix_out[t] = dot(gained, w_out[:, of_tp(t)]).astype(BF16)
        send(mix_out.at[t], mix_in.at[tp], mxs.at[k], mxr.at[tp], along_tp(k))
        send(energy.at[tp], energy.at[tp], ens.at[k], enr.at[tp], along_tp(k))
    mix = dot(gained, w_out[:, of_tp(tp)])
    wgt_pass(2, 0)
    wgt_pass(2, 1)
    for k in order:
        t = wrap(tp + k)
        arrived(mix_in.at[t], mxr.at[t])
        arrived(energy.at[t], enr.at[t])
        mix = mix + mix_in[t].astype(F32)
    power = energy[0]
    for t in range(1, N):
        power = power + energy[t]
    factor = lax.rsqrt(power[0:1] / (HA * DA + HB * DB) + EPS_RMS)
    factor = jnp.broadcast_to(factor, (ROWS, ROWS)).T[:, 0:1]
    pre[tp] = (ALPHA * resid[...].astype(F32) + mix * factor).astype(BF16)
    for k in order:
        send(pre.at[tp], pre.at[tp], prs.at[k], prr.at[tp], along_tp(k))
    wgt_pass(2, 2)
    wgt_pass(2, 3)
    wgt_pass(3, 0, True, False)
    wgt_pass(3, 2, False, True)
    for k in order:
        t = wrap(tp + k)
        arrived(pre.at[t], prr.at[t])

    center = jnp.sum(pre[0].astype(F32), axis=1, keepdims=True)
    for t in range(1, N):
        center = center + jnp.sum(pre[t].astype(F32), axis=1, keepdims=True)
    center = center / D
    spread = jnp.zeros((ROWS, 1), F32)
    for t in range(N):
        shifted = pre[t].astype(F32) - center
        spread = spread + jnp.sum(shifted * shifted, axis=1, keepdims=True)
    scale = lax.rsqrt(spread / D + EPS_NORM)

    def normed_cols(t):
        return ((pre[t].astype(F32) - center) * scale * norm1_gain[:, t * COLS : (t + 1) * COLS]).astype(BF16)

    own = (pre[tp].astype(F32) - center) * scale * norm1_gain[:, of_tp(tp)]
    first_own[...] = own.astype(BF16)

    @pl.when(core == 0)
    def _():
        for t in range(N):
            first[HALO:, t * COLS : (t + 1) * COLS] = normed_cols(t)

    @pl.when(core == 1)
    def _():
        for t in range(N):
            value = normed_cols(t)
            for g in range(N):
                first[HALO:, g * COLS + t * 32 : g * COLS + (t + 1) * 32] = value[:, g * 32 : (g + 1) * 32]

    send(first.at[ROWS : ROWS + HALO], first.at[0:HALO], hls.at[0], hlr.at[0], nxt)
    wgt_pass(3, 1, True, False)
    wgt_pass(3, 3, False, True)
    arrived(first.at[0:HALO], hlr.at[0])

    def project(i):
        b = wrap(beta + offset(i))
        return dot(first[:, of_tp(b)], wgt[b].reshape(COLS, 2 * UNITS))

    def project_more(begin, end):
        def body(i, carry):
            up[...] += project(i)
            return carry

        lax.fori_loop(begin, end, body, 0)

    up[...] = jnp.zeros_like(up)
    project_more(0, 5)
    for b, p in (
        (wrap(beta + N - 3), 2),
        (wrap(beta + N - 3), 3),
        (wrap(beta + 3), 0),
        (wrap(beta + 3), 1),
    ):
        arrived(wgt_piece(b, p), w2r.at[4 * b + p])
    project_more(5, 7)
    b = wrap(beta + 4)
    for p in range(4):
        arrived(wgt_piece(b, p), w2r.at[4 * b + p])
    project_more(7, 8)

    up[...] = up[...].astype(BF16).astype(F32)

    @pl.when(sp == 0)
    def _():
        up[0:HALO, :] = jnp.zeros((HALO, 2 * UNITS), F32)

    def conv(taps, at, width):
        value = taps[0:1] * up[HALO - 2 : HALO - 2 + ROWS, at : at + width]
        value = value + taps[1:2] * up[HALO - 1 : HALO - 1 + ROWS, at : at + width]
        return value + taps[2:3] * up[HALO : HALO + ROWS, at : at + width]

    def gated(g, v):
        return (g / (1.0 + jnp.exp(-g)) * v).astype(BF16)

    for at in range(0, MAIN, 128):
        g = conv(conv_gate[:, at : at + 128], at, 128)
        v = conv(conv_val[:, at : at + 128], MAIN + at, 128)
        hidden[:, at : at + 128] = gated(g, v)
    taps = jnp.concatenate([conv_gate[:, MAIN:], conv_val[:, MAIN:]], axis=1)
    both = conv(taps, 2 * MAIN, 128)
    hidden[:, MAIN:] = gated(both[:, :64], both[:, 64:])

    local[2].wait()
    for k in order:
        t = wrap(tp + k)
        down_out[t] = dot(hidden[...], w_down[:, of_tp(t)]).astype(BF16)
        send(down_out.at[t], down_in.at[tp], dns.at[k], dnr.at[tp], along_tp(k))
    value = dot(hidden[...], w_down[:, of_tp(tp)]) + ALPHA * first_own[...].astype(F32)
    for k in order:
        t = wrap(tp + k)
        arrived(down_in.at[t], dnr.at[t])
        value = value + down_in[t].astype(F32)

    amount = jnp.sum(value, axis=1, keepdims=True)
    apart = value - amount / COLS
    apart = jnp.sum(apart * apart, axis=1, keepdims=True)
    line = lax.broadcasted_iota(jnp.int32, (8, ROWS), 0)
    stats[tp] = jnp.where(
        line == 0,
        jnp.broadcast_to(amount, (ROWS, ROWS)).T[0:8],
        jnp.broadcast_to(apart, (ROWS, ROWS)).T[0:8],
    )
    for k in order:
        send(stats.at[tp], stats.at[tp], sts.at[k], srr.at[tp], along_tp(k))
    for k in order:
        t = wrap(tp + k)
        arrived(stats.at[t], srr.at[t])
    whole = stats[0]
    for t in range(1, N):
        whole = whole + stats[t]
    center = whole[0:1] / D
    spread = whole[1:2]
    for t in range(N):
        gap = stats[t][0:1] / COLS - center
        spread = spread + COLS * gap * gap
    scale = lax.rsqrt(spread / D + EPS_NORM)
    center = jnp.broadcast_to(center, (ROWS, ROWS)).T[:, 0:1]
    scale = jnp.broadcast_to(scale, (ROWS, ROWS)).T[:, 0:1]
    out[...] = ((value - center) * scale * norm2_gain[...]).astype(BF16)

    for copy in pending:
        copy.wait_send()


def shards(*args):
    (
        resid,
        qa_nope,
        qb_nope,
        qa_rope,
        qb_rope,
        latent,
        key_rope,
        lat_gain,
        wa_key,
        wa_val,
        wb_key,
        wb_val,
        gain_a,
        gain_b,
        wa_out,
        wb_out,
        norm1_gain,
        ffn_gate,
        ffn_val,
        conv_gate,
        conv_val,
        ffn_down,
        norm2_gain,
    ) = args
    positions = lax.axis_index("sp") * ROWS + jnp.arange(ROWS)
    freq = THETA ** (-jnp.arange(DR // 2, dtype=F32) * 2.0 / DR)
    angle = positions.astype(F32)[:, None] * jnp.concatenate([freq, freq])[None, :]
    cosine = jnp.cos(angle)
    sign = jnp.where(jnp.arange(DR) < DR // 2, -1.0, 1.0).astype(F32)
    sine = jnp.sin(angle) * sign[None, :]
    vmem = pl.BlockSpec(memory_space=pltpu.VMEM)
    anywhere = pl.BlockSpec(memory_space=pl.ANY)
    operands = (
        cosine,
        sine,
        resid,
        qa_nope,
        qb_nope,
        qa_rope,
        qb_rope,
        latent,
        key_rope,
        lat_gain[None],
        wa_key,
        wa_val,
        wb_key,
        wb_val,
        gain_a[None],
        gain_b[None],
        wa_out,
        wb_out,
        norm1_gain[None],
        ffn_gate,
        ffn_val,
        conv_gate,
        conv_val,
        ffn_down,
        norm2_gain[None],
    )
    specs = [vmem] * len(operands)
    for at in (16, 17, 23):
        specs[at] = anywhere
    dma = pltpu.SemaphoreType.DMA
    return pl.pallas_call(
        kernel,
        out_shape=jax.ShapeDtypeStruct((ROWS, COLS), BF16),
        in_specs=specs,
        out_specs=vmem,
        scratch_shapes=[
            pltpu.VMEM((2, N, N, 144, 128), BF16),
            pltpu.VMEM((N, N, 32, 2 * UNITS), BF16),
            pltpu.VMEM((3 * ROWS, LAT), BF16),
            pltpu.VMEM((3 * ROWS, DR), BF16),
            pltpu.VMEM((3 * ROWS, LAT), F32),
            pltpu.VMEM((3 * ROWS, 128), F32),
            pltpu.VMEM((3 * ROWS, 128), F32),
            pltpu.VMEM((256, D), BF16),
            pltpu.VMEM((UNITS, D), BF16),
            pltpu.VMEM((N, ROWS, COLS), BF16),
            pltpu.VMEM((N, ROWS, COLS), BF16),
            pltpu.VMEM((N, 8, ROWS), F32),
            pltpu.VMEM((N, ROWS, COLS), BF16),
            pltpu.VMEM((HALO + ROWS, D), BF16),
            pltpu.VMEM((ROWS, COLS), BF16),
            pltpu.VMEM((HALO + ROWS, 2 * UNITS), F32),
            pltpu.VMEM((ROWS, UNITS), BF16),
            pltpu.VMEM((N, ROWS, COLS), BF16),
            pltpu.VMEM((N, ROWS, COLS), BF16),
            pltpu.VMEM((N, 8, ROWS), F32),
            dma((3,)),
            dma((7,)),
            dma((8,)),
            dma((8,)),
            dma((8,)),
            dma((14,)),
            dma((16,)),
            dma((8,)),
            dma((8,)),
            dma((28,)),
            dma((32,)),
            dma((8,)),
            dma((8,)),
            dma((8,)),
            dma((8,)),
            dma((8,)),
            dma((8,)),
            dma((1,)),
            dma((1,)),
            dma((8,)),
            dma((8,)),
            dma((8,)),
            dma((8,)),
        ],
        compiler_params=pltpu.CompilerParams(
            collective_id=0, has_side_effects=True, vmem_limit_bytes=56 * 1024 * 1024
        ),
        cost_estimate=pl.CostEstimate(flops=8_000_000_000, bytes_accessed=20_000_000, transcendentals=4_000_000),
    )(*operands)


def solution(mesh):
    return jax.shard_map(
        shards,
        mesh=mesh,
        in_specs=(
            P("sp", "tp"),
            P("sp", "tp"),
            P("sp", "tp"),
            P("sp", "tp"),
            P("sp", "tp"),
            P("sp", None),
            P("sp", None),
            P(),
            P(None, "tp"),
            P(None, "tp"),
            P(None, "tp"),
            P(None, "tp"),
            P("tp"),
            P("tp"),
            P("tp", None),
            P("tp", None),
            P(),
            P("sp", "tp"),
            P("sp", "tp"),
            P(None, "tp"),
            P(None, "tp"),
            P("tp", None),
            P("tp"),
        ),
        out_specs=P("sp", "tp"),
        check_vma=False,
    )
```

```python
import jax
import jax.numpy as jnp
import numpy as np
from jax import lax
from jax.experimental import pallas as pl
from jax.experimental.pallas import tpu as pltpu
from jax.sharding import PartitionSpec as P

D = 2048
HA = 16
DA = 64
HB = 8
DB = 128
DR = 32
LAT = 256
KC = 3
ROWS = 128
COLS = 256
UNITS = 704
MAIN = 640
HALO = 16
N = 8

THETA = 10000.0
EPS_RMS = 1e-06
EPS_NORM = 1e-05
ALPHA = 2.0**0.25
LOG2E = 1.4426950408889634
LOW = -1e30
MESH = pl.DeviceIdType.MESH
F32 = jnp.float32
BF16 = jnp.bfloat16


def dot(a, b):
    return jnp.dot(a, b, preferred_element_type=F32)


def dot_t(a, b):
    return lax.dot_general(a, b, (((1,), (1,)), ((), ())), preferred_element_type=F32)


class Stages:
    def __init__(self):
        self.scope = None

    def __call__(self, name):
        if self.scope is not None:
            self.scope.__exit__(None, None, None)
        self.scope = None
        if name:
            self.scope = jax.named_scope(name)
            self.scope.__enter__()


def wrap(v):
    return lax.rem(v, N)


def kernel(
    freq,
    resid,
    qa_nope,
    qb_nope,
    qa_rope,
    qb_rope,
    latent,
    key_rope,
    lat_gain,
    wa_key,
    wa_val,
    wb_key,
    wb_val,
    gain_a,
    gain_b,
    wa_out,
    wb_out,
    norm1_gain,
    ffn_gate,
    ffn_val,
    conv_gate,
    conv_val,
    ffn_down,
    norm2_gain,
    out,
    lat,
    wgt,
    q_lat,
    q_rot,
    acc,
    top,
    total,
    w_out,
    w_down,
    mix_out,
    mix_in,
    energy,
    pre,
    pre_halo,
    first,
    first_own,
    up,
    hidden,
    down_out,
    down_in,
    stats,
    local_sem,
    l1s,
    l1r,
    w1s,
    w1r,
    l2s,
    l2r,
    dds,
    ddr,
    xss,
    xsr,
    xds,
    xdr,
    w2s,
    w2r,
    mxs,
    mxr,
    ens,
    enr,
    prs,
    prr,
    hls,
    hlr,
    dns,
    dnr,
    sts,
    srr,
):
    stage = Stages()
    stage("enter")
    sp = lax.axis_index("sp")
    tp = lax.axis_index("tp")
    core = lax.rem(tp, 2)
    z = lax.div(sp, N)
    y = lax.rem(sp, N)
    alpha = y + core * (z - y)
    beta = z + core * (y - z)
    sa = 1 + 7 * core
    sb = 8 - 7 * core
    partner = (sp, tp + 1 - 2 * core)
    sideways = (sp, wrap(tp + 2 + 4 * core))
    parity = lax.rem(lax.div(tp, 2), 2)
    part_of = 2 * parity + core
    nxt = (lax.rem(sp + 1, N * N), tp)
    prv = (lax.rem(sp + N * N - 1, N * N), tp)

    def along_a(k):
        return (wrap(alpha + k) * sa + beta * sb, tp)

    def along_b(k):
        return (alpha * sa + wrap(beta + k) * sb, tp)

    def along_tp(k):
        return (sp, wrap(tp + k))

    def remote(src, dst, send, recv, device):
        return pltpu.make_async_remote_copy(
            src_ref=src, dst_ref=dst, send_sem=send, recv_sem=recv, device_id=device, device_id_type=MESH
        )

    pending = []

    def send(src, dst, ssem, rsem, device):
        copy = remote(src, dst, ssem, rsem, device)
        copy.start()
        pending.append(copy)

    def arrived(ref, rsem):
        remote(ref, ref, l1s.at[0], rsem, partner).wait_recv()

    barrier = pltpu.get_barrier_semaphore()
    peers = [along_a(k) for k in range(1, N)] + [along_b(1), along_b(N - 1)]
    peers += [along_tp(k) for k in range(1, N)]
    peers += [(line[0], t) for line in (nxt, prv) for t in range(N)]
    for device in peers:
        pl.semaphore_signal(barrier, inc=1, device_id=device, device_id_type=MESH)

    local = [
        pltpu.make_async_copy(wa_out, w_out.at[0:128], local_sem.at[0]),
        pltpu.make_async_copy(wb_out, w_out.at[128:256], local_sem.at[1]),
        pltpu.make_async_copy(ffn_down, w_down, local_sem.at[2]),
    ]
    for copy in local:
        copy.start()

    stage("prep")
    quarter = pl.ds(pl.multiple_of(part_of * 32, 32), 32)
    wide = latent[quarter, :].astype(F32)
    wide = wide * lax.rsqrt(jnp.mean(wide * wide, axis=1, keepdims=True) + EPS_RMS) * lat_gain[...]
    lat_n = wide.astype(BF16)

    spots = sp * ROWS + lax.broadcasted_iota(jnp.int32, (DR // 2, ROWS), 1)
    angle = spots.astype(F32) * freq[...]
    cosine = jnp.cos(angle)
    sine = jnp.sin(angle)

    def rotated(v):
        a = v[: DR // 2].astype(F32)
        b = v[DR // 2 :].astype(F32)
        return jnp.concatenate([a * cosine - b * sine, b * cosine + a * sine], axis=0)

    k_t = rotated(key_rope[...])
    k_packed = jnp.zeros((8, 128), F32)
    for q in range(4):
        taken = [k_t[8 * g : 8 * g + 8, 32 * q : 32 * q + 32] for g in range(4)]
        k_packed = jnp.where(part_of == q, jnp.concatenate(taken, axis=1), k_packed)
    lat[core, beta, alpha, 0:32, :] = lat_n[:, :128]
    lat[core, beta, alpha, 32:64, :] = lat_n[:, 128:]
    lat[core, beta, alpha, 64:80, :] = jnp.concatenate([k_packed, k_packed], axis=0).astype(BF16)
    wgt[beta, alpha, :, 0:MAIN] = ffn_gate[:, :MAIN]
    wgt[beta, alpha, :, MAIN : 2 * MAIN] = ffn_val[:, :MAIN]
    wgt[beta, alpha, :, 2 * MAIN :] = jnp.concatenate(
        [ffn_gate[:, MAIN:].astype(F32), ffn_val[:, MAIN:].astype(F32)], axis=1
    ).astype(BF16)

    stage("barrier")
    pl.semaphore_wait(barrier, len(peers))

    stage("send1")
    mine = lat.at[core, beta, alpha]
    for k in (4, 3, 5, 2, 6, 1, 7):
        send(mine, mine, l1s.at[k - 1], l1r.at[alpha], along_a(k))

    def weight_step(step, forward, backward):
        if forward:
            block = wgt.at[beta, wrap(alpha + N - step)]
            if step:
                arrived(block, w1r.at[wrap(alpha + N - step)])
            send(block, block, w1s.at[step], w1r.at[wrap(alpha + N - step)], along_a(1))
        if backward:
            block = wgt.at[beta, wrap(alpha + step)]
            if step:
                arrived(block, w1r.at[wrap(alpha + step)])
            send(block, block, w1s.at[4 + step], w1r.at[wrap(alpha + step)], along_a(N - 1))

    weight_step(0, True, True)

    stage("queries")
    q_scale_a = (DA + DR) ** (-0.5) * LOG2E
    q_scale_b = (DB + DR) ** (-0.5) * LOG2E
    for h in range(2):
        part = dot_t(qa_nope[:, h * DA : (h + 1) * DA], wa_key[:, h * DA : (h + 1) * DA])
        q_lat[h * ROWS : (h + 1) * ROWS, :] = (part * q_scale_a).astype(BF16)
    part = dot_t(qb_nope[...], wb_key[...])
    q_lat[2 * ROWS :, :] = (part * q_scale_b).astype(BF16)
    turned = [rotated(qa_rope[h * DR : (h + 1) * DR]) * q_scale_a for h in range(2)]
    turned += [rotated(qb_rope[...]) * q_scale_b, jnp.zeros((DR, ROWS), F32)]
    turned = jnp.concatenate(turned, axis=0).T.astype(BF16)
    for h in range(3):
        q_rot[h * ROWS : (h + 1) * ROWS, :] = turned[:, h * DR : (h + 1) * DR]
    acc[...] = jnp.zeros_like(acc)
    top[...] = jnp.full_like(top, LOW)
    total[...] = jnp.zeros_like(total)

    def offset(i):
        steps = lax.div(i + 1, 2)
        return wrap(N + steps * (1 - 2 * lax.rem(i, 2)))

    def lat_piece(b, p):
        return lat.at[core, b, pl.ds(4 * p, 4)]

    def lat_pass(d, p, forward, backward):
        for go, b, k, base in (
            (forward, wrap(beta + N - d), 1, 0),
            (backward, wrap(beta + d), N - 1, 7),
        ):
            if go:
                if d:
                    arrived(lat_piece(b, p), l2r.at[2 * b + p])
                at = base + (2 * d + p if d < 3 else 6)
                send(lat_piece(b, p), lat_piece(b, p), l2s.at[at], l2r.at[2 * b + p], along_b(k))

    def hand_over(b):
        send(lat.at[core, b], lat.at[3 - core, b], xss.at[b], xsr.at[b], sideways)
        send(lat.at[core, b], lat.at[core, b], dds.at[b], ddr.at[b], partner)

    def pass_over(i):
        b = wrap(beta + offset(i))
        block = lat.at[3 - core, b]
        arrived(block, xsr.at[b])
        send(block, block, xds.at[b], xdr.at[b], partner)

    def wgt_piece(b, p):
        return wgt.at[b, pl.ds(2 * p, 2)]

    def wgt_pass(d, p, forward=True, backward=True):
        for go, b, k, base in (
            (forward, wrap(beta + N - d), 1, 0),
            (backward, wrap(beta + d), N - 1, 14),
        ):
            if go:
                if d:
                    arrived(wgt_piece(b, p), w2r.at[4 * b + p])
                at = base + 4 * d + (p if d < 3 or k == 1 else p - 2)
                send(wgt_piece(b, p), wgt_piece(b, p), w2s.at[at], w2r.at[4 * b + p], along_b(k))

    def attend(i):
        b0 = wrap(z + offset(i))
        b1 = wrap(y + offset(i))
        theirs = wrap(alpha + offset(i))
        arrived(lat.at[1 - core, theirs], ddr.at[theirs])
        arrived(lat.at[2 + core, theirs], xdr.at[theirs])
        left, right, roped = [], [], []
        for slot, b in ((0, b0), (1, b1), (2, b1), (3, b0)):
            left.append(lat[slot, b, :, 0:32, :].reshape(256, 128))
            right.append(lat[slot, b, :, 32:64, :].reshape(256, 128))
            x = lat[slot, b, :, 64:80, :].astype(F32)
            for quad in range(0, N, 4):
                lines = [
                    jnp.concatenate([x[a][0:8, 32 * g : 32 * g + 32] for a in range(quad, quad + 4)], axis=1)
                    for g in range(4)
                ]
                roped.append(jnp.concatenate(lines, axis=0).astype(BF16))
        keys = jnp.concatenate(
            [jnp.concatenate(left, axis=0), jnp.concatenate(right, axis=0)], axis=1
        )
        ropes = jnp.concatenate(roped, axis=1)
        scores = dot_t(q_lat[...], keys) + dot(q_rot[...], ropes)
        j = lax.broadcasted_iota(jnp.int32, (1, 1024), 1)
        slot = lax.shift_right_logical(j, 8)
        a = lax.bitwise_and(lax.shift_right_logical(j, 5), 7)
        r = lax.bitwise_and(j, 31)
        block = jnp.where((slot == 0) | (slot == 3), b0 * N + a, a * N + b1)
        which = jnp.where(slot < 2, 2 * parity + slot, 5 - 2 * parity - slot)
        spots = block * ROWS + which * 32 + r
        rows = lax.broadcasted_iota(jnp.int32, (3 * ROWS, 1), 0)
        rows = sp * ROWS + lax.bitwise_and(rows, ROWS - 1)
        scores = jnp.where(spots <= rows, scores, LOW)
        old = top[:, 0:1]
        new = jnp.maximum(old, jnp.max(scores, axis=1, keepdims=True))
        weights = jnp.exp2(scores - new)
        shrink = jnp.exp2(old - new)
        total[...] = total[...] * shrink + jnp.sum(weights, axis=1, keepdims=True)
        acc[...] = acc[...] * shrink + dot(weights.astype(BF16), keys)
        top[...] = jnp.broadcast_to(new, top.shape)

    stage("lat1")
    for k in range(1, N):
        block = lat.at[core, beta, wrap(alpha + k)]
        arrived(block, l1r.at[wrap(alpha + k)])
    stage("ring0")
    lat_pass(0, 0, True, True)
    lat_pass(0, 1, True, True)
    hand_over(beta)
    stage("w1_1")
    weight_step(1, True, True)
    stage("ring1a")
    lat_pass(1, 0, True, True)
    stage("ring1b")
    lat_pass(1, 1, True, True)
    hand_over(wrap(beta + N - 1))
    hand_over(wrap(beta + 1))
    stage("over0")
    pass_over(0)
    stage("w1_2")
    weight_step(2, True, True)
    stage("attend0")
    attend(0)
    stage("ring2a")
    lat_pass(2, 0, True, True)
    stage("ring2b")
    lat_pass(2, 1, True, True)
    hand_over(wrap(beta + N - 2))
    hand_over(wrap(beta + 2))
    stage("w1_3")
    weight_step(3, True, False)
    stage("over1")
    pass_over(1)
    stage("over2")
    pass_over(2)
    stage("attend1")
    attend(1)
    stage("ring3")
    lat_pass(3, 0, True, False)
    lat_pass(3, 1, False, True)
    stage("w1_4")
    for k in (3, 4):
        a = wrap(alpha + k)
        arrived(wgt.at[beta, a], w1r.at[a])
    wgt_pass(0, 0)
    wgt_pass(0, 1)
    stage("attend2")
    attend(2)
    stage("ring3end")
    for b, p in ((wrap(beta + N - 3), 1), (wrap(beta + 3), 0)):
        arrived(lat_piece(b, p), l2r.at[2 * b + p])
    hand_over(wrap(beta + N - 3))
    hand_over(wrap(beta + 3))
    stage("over3")
    pass_over(3)
    wgt_pass(0, 2)
    stage("ring4")
    b = wrap(beta + 4)
    arrived(lat_piece(b, 0), l2r.at[2 * b])
    arrived(lat_piece(b, 1), l2r.at[2 * b + 1])
    hand_over(b)
    wgt_pass(0, 3)
    stage("over4")
    pass_over(4)
    stage("attend3")
    attend(3)
    stage("pass1_0")
    wgt_pass(1, 0)
    stage("over5")
    pass_over(5)
    stage("attend4")
    attend(4)
    stage("pass1_1")
    wgt_pass(1, 1)
    stage("over6")
    pass_over(6)
    stage("attend5")
    attend(5)
    stage("pass1_2")
    wgt_pass(1, 2)
    stage("over7")
    pass_over(7)
    stage("attend6")
    attend(6)
    stage("pass1_3")
    wgt_pass(1, 3)
    stage("attend7")
    attend(7)
    stage("pass2_0")
    wgt_pass(2, 0)
    stage("heads")
    normed = (acc[...] / total[:, 0:1]).astype(BF16)
    raw_a = jnp.concatenate(
        [dot(normed[h * ROWS : (h + 1) * ROWS], wa_val[:, h * DA : (h + 1) * DA]) for h in range(2)], axis=1
    )
    raw_b = dot(normed[2 * ROWS :], wb_val[...])
    power = jnp.sum(raw_a * raw_a, axis=1, keepdims=True) + jnp.sum(raw_b * raw_b, axis=1, keepdims=True)
    energy[tp] = jnp.broadcast_to(power, (ROWS, ROWS)).T[0:8]
    gained = jnp.concatenate([raw_a * gain_a[...], raw_b * gain_b[...]], axis=1).astype(BF16)
    local[0].wait()
    local[1].wait()

    def of_tp(t):
        return pl.ds(pl.multiple_of(t * COLS, COLS), COLS)

    stage("mixsend")
    order = (4, 5, 3, 2, 6, 7, 1)
    for k in order:
        t = wrap(tp + k)
        mix_out[t] = dot(gained, w_out[:, of_tp(t)]).astype(BF16)
        send(mix_out.at[t], mix_in.at[tp], mxs.at[k], mxr.at[tp], along_tp(k))
        send(energy.at[tp], energy.at[tp], ens.at[k], enr.at[tp], along_tp(k))
    mix = dot(gained, w_out[:, of_tp(tp)])
    stage("pass2_123")
    wgt_pass(2, 1)
    wgt_pass(2, 2)
    wgt_pass(2, 3)
    stage("mixwait")
    for k in order:
        t = wrap(tp + k)
        arrived(mix_in.at[t], mxr.at[t])
        arrived(energy.at[t], enr.at[t])
        mix = mix + mix_in[t].astype(F32)
    stage("mixsum")
    power = energy[0]
    for t in range(1, N):
        power = power + energy[t]
    factor = lax.rsqrt(power[0:1] / (HA * DA + HB * DB) + EPS_RMS)
    factor = jnp.broadcast_to(factor, (ROWS, ROWS)).T[:, 0:1]
    pre[tp] = (ALPHA * resid[...].astype(F32) + mix * factor).astype(BF16)
    for k in (4, 2, 6):
        send(pre.at[tp], pre.at[tp], prs.at[k], prr.at[tp], along_tp(k))
    send(pre.at[tp], pre.at[tp], prs.at[1], prr.at[tp], partner)
    for t in range(N):
        send(pre.at[tp, ROWS - HALO : ROWS], pre_halo.at[tp], hls.at[t], hlr.at[tp], (nxt[0], t))
    stage("pass3")
    wgt_pass(3, 0, True, False)
    wgt_pass(3, 2, False, True)
    wgt_pass(3, 1, True, False)
    wgt_pass(3, 3, False, True)
    stage("prewait")
    for k in (2, 6, 4):
        t = wrap(tp + k)
        arrived(pre.at[t], prr.at[t])
        send(pre.at[t], pre.at[t], prs.at[k + 1], prr.at[t], partner)
    stage("halowait")
    for t in range(N):
        arrived(pre_halo.at[t], hlr.at[t])
    stage("prewait2")
    for k in (1, 3, 5, 7):
        t = wrap(tp + k)
        arrived(pre.at[t], prr.at[t])

    stage("norm1")
    def row_stats(ref):
        middle = jnp.sum(ref[0].astype(F32), axis=1, keepdims=True)
        for t in range(1, N):
            middle = middle + jnp.sum(ref[t].astype(F32), axis=1, keepdims=True)
        middle = middle / D
        wide = jnp.zeros_like(middle)
        for t in range(N):
            shifted = ref[t].astype(F32) - middle
            wide = wide + jnp.sum(shifted * shifted, axis=1, keepdims=True)
        return middle, lax.rsqrt(wide / D + EPS_NORM)

    center, scale = row_stats(pre)
    center_halo, scale_halo = row_stats(pre_halo)

    def normed_cols(t):
        gain = norm1_gain[:, t * COLS : (t + 1) * COLS]
        above = (pre_halo[t].astype(F32) - center_halo) * scale_halo * gain
        return jnp.concatenate([above, (pre[t].astype(F32) - center) * scale * gain], axis=0).astype(BF16)

    own = (pre[tp].astype(F32) - center) * scale * norm1_gain[:, of_tp(tp)]
    first_own[...] = own.astype(BF16)

    @pl.when(core == 0)
    def _():
        for t in range(N):
            first[:, t * COLS : (t + 1) * COLS] = normed_cols(t)

    @pl.when(core == 1)
    def _():
        for t in range(N):
            value = normed_cols(t)
            for g in range(N):
                first[:, g * COLS + t * 32 : g * COLS + (t + 1) * 32] = value[:, g * 32 : (g + 1) * 32]

    def project(i):
        b = wrap(beta + offset(i))
        return dot(first[:, of_tp(b)], wgt[b].reshape(COLS, 2 * UNITS))

    def project_more(begin, end):
        def body(i, carry):
            up[...] += project(i)
            return carry

        lax.fori_loop(begin, end, body, 0)

    stage("up5")
    up[...] = jnp.zeros_like(up)
    project_more(0, 5)
    stage("wait3")
    for b, p in (
        (wrap(beta + N - 3), 2),
        (wrap(beta + N - 3), 3),
        (wrap(beta + 3), 0),
        (wrap(beta + 3), 1),
    ):
        arrived(wgt_piece(b, p), w2r.at[4 * b + p])
    stage("up7")
    project_more(5, 7)
    stage("wait4")
    b = wrap(beta + 4)
    for p in range(4):
        arrived(wgt_piece(b, p), w2r.at[4 * b + p])
    stage("up8")
    project_more(7, 8)

    stage("conv")
    up[...] = up[...].astype(BF16).astype(F32)

    @pl.when(sp == 0)
    def _():
        up[0:HALO, :] = jnp.zeros((HALO, 2 * UNITS), F32)

    def conv(taps, at, width):
        value = taps[0:1] * up[HALO - 2 : HALO - 2 + ROWS, at : at + width]
        value = value + taps[1:2] * up[HALO - 1 : HALO - 1 + ROWS, at : at + width]
        return value + taps[2:3] * up[HALO : HALO + ROWS, at : at + width]

    def gated(g, v):
        return (g / (1.0 + jnp.exp(-g)) * v).astype(BF16)

    for at in range(0, MAIN, 128):
        g = conv(conv_gate[:, at : at + 128], at, 128)
        v = conv(conv_val[:, at : at + 128], MAIN + at, 128)
        hidden[:, at : at + 128] = gated(g, v)
    taps = jnp.concatenate([conv_gate[:, MAIN:], conv_val[:, MAIN:]], axis=1)
    both = conv(taps, 2 * MAIN, 128)
    hidden[:, MAIN:] = gated(both[:, :64], both[:, 64:])

    stage("down")
    local[2].wait()
    for k in order:
        t = wrap(tp + k)
        down_out[t] = dot(hidden[...], w_down[:, of_tp(t)]).astype(BF16)
        send(down_out.at[t], down_in.at[tp], dns.at[k], dnr.at[tp], along_tp(k))
    value = dot(hidden[...], w_down[:, of_tp(tp)]) + ALPHA * first_own[...].astype(F32)
    stage("downwait")
    for k in order:
        t = wrap(tp + k)
        arrived(down_in.at[t], dnr.at[t])
        value = value + down_in[t].astype(F32)

    stage("stats")
    amount = jnp.sum(value, axis=1, keepdims=True)
    apart = value - amount / COLS
    apart = jnp.sum(apart * apart, axis=1, keepdims=True)
    line = lax.broadcasted_iota(jnp.int32, (8, ROWS), 0)
    stats[tp] = jnp.where(
        line == 0,
        jnp.broadcast_to(amount, (ROWS, ROWS)).T[0:8],
        jnp.broadcast_to(apart, (ROWS, ROWS)).T[0:8],
    )
    for k in order:
        send(stats.at[tp], stats.at[tp], sts.at[k], srr.at[tp], along_tp(k))
    stage("statswait")
    for k in order:
        t = wrap(tp + k)
        arrived(stats.at[t], srr.at[t])
    stage("finish")
    whole = stats[0]
    for t in range(1, N):
        whole = whole + stats[t]
    center = whole[0:1] / D
    spread = whole[1:2]
    for t in range(N):
        gap = stats[t][0:1] / COLS - center
        spread = spread + COLS * gap * gap
    scale = lax.rsqrt(spread / D + EPS_NORM)
    center = jnp.broadcast_to(center, (ROWS, ROWS)).T[:, 0:1]
    scale = jnp.broadcast_to(scale, (ROWS, ROWS)).T[:, 0:1]
    out[...] = ((value - center) * scale * norm2_gain[...]).astype(BF16)

    stage("drain")
    for copy in pending:
        copy.wait_send()
    stage(None)


def shards(*args):
    (
        resid,
        qa_nope,
        qb_nope,
        qa_rope,
        qb_rope,
        latent,
        key_rope,
        lat_gain,
        wa_key,
        wa_val,
        wb_key,
        wb_val,
        gain_a,
        gain_b,
        wa_out,
        wb_out,
        norm1_gain,
        ffn_gate,
        ffn_val,
        conv_gate,
        conv_val,
        ffn_down,
        norm2_gain,
    ) = args
    freq = np.float64(THETA) ** (-np.arange(DR // 2) * 2.0 / DR)
    freq = jnp.asarray(np.broadcast_to(freq[:, None], (DR // 2, ROWS)).astype(np.float32))
    vmem = pl.BlockSpec(memory_space=pltpu.VMEM)
    anywhere = pl.BlockSpec(memory_space=pl.ANY)
    operands = (
        freq,
        resid,
        qa_nope,
        qb_nope,
        qa_rope.T,
        qb_rope.T,
        latent,
        key_rope.T,
        lat_gain[None],
        wa_key,
        wa_val,
        wb_key,
        wb_val,
        gain_a[None],
        gain_b[None],
        wa_out,
        wb_out,
        norm1_gain[None],
        ffn_gate,
        ffn_val,
        conv_gate,
        conv_val,
        ffn_down,
        norm2_gain[None],
    )
    specs = [vmem] * len(operands)
    for at in (15, 16, 22):
        specs[at] = anywhere
    dma = pltpu.SemaphoreType.DMA
    return pl.pallas_call(
        kernel,
        out_shape=jax.ShapeDtypeStruct((ROWS, COLS), BF16),
        in_specs=specs,
        out_specs=vmem,
        scratch_shapes=[
            pltpu.VMEM((4, N, N, 80, 128), BF16),
            pltpu.VMEM((N, N, 32, 2 * UNITS), BF16),
            pltpu.VMEM((3 * ROWS, LAT), BF16),
            pltpu.VMEM((3 * ROWS, DR), BF16),
            pltpu.VMEM((3 * ROWS, LAT), F32),
            pltpu.VMEM((3 * ROWS, 128), F32),
            pltpu.VMEM((3 * ROWS, 128), F32),
            pltpu.VMEM((256, D), BF16),
            pltpu.VMEM((UNITS, D), BF16),
            pltpu.VMEM((N, ROWS, COLS), BF16),
            pltpu.VMEM((N, ROWS, COLS), BF16),
            pltpu.VMEM((N, 8, ROWS), F32),
            pltpu.VMEM((N, ROWS, COLS), BF16),
            pltpu.VMEM((N, HALO, COLS), BF16),
            pltpu.VMEM((HALO + ROWS, D), BF16),
            pltpu.VMEM((ROWS, COLS), BF16),
            pltpu.VMEM((HALO + ROWS, 2 * UNITS), F32),
            pltpu.VMEM((ROWS, UNITS), BF16),
            pltpu.VMEM((N, ROWS, COLS), BF16),
            pltpu.VMEM((N, ROWS, COLS), BF16),
            pltpu.VMEM((N, 8, ROWS), F32),
            dma((3,)),
            dma((7,)),
            dma((8,)),
            dma((8,)),
            dma((8,)),
            dma((14,)),
            dma((16,)),
            dma((8,)),
            dma((8,)),
            dma((8,)),
            dma((8,)),
            dma((8,)),
            dma((8,)),
            dma((28,)),
            dma((32,)),
            dma((8,)),
            dma((8,)),
            dma((8,)),
            dma((8,)),
            dma((8,)),
            dma((8,)),
            dma((8,)),
            dma((8,)),
            dma((8,)),
            dma((8,)),
            dma((8,)),
            dma((8,)),
        ],
        compiler_params=pltpu.CompilerParams(
            collective_id=0, has_side_effects=True, vmem_limit_bytes=56 * 1024 * 1024
        ),
        cost_estimate=pl.CostEstimate(flops=8_000_000_000, bytes_accessed=20_000_000, transcendentals=4_000_000),
    )(*operands)


def solution(mesh):
    return jax.shard_map(
        shards,
        mesh=mesh,
        in_specs=(
            P("sp", "tp"),
            P("sp", "tp"),
            P("sp", "tp"),
            P("sp", "tp"),
            P("sp", "tp"),
            P("sp", None),
            P("sp", None),
            P(),
            P(None, "tp"),
            P(None, "tp"),
            P(None, "tp"),
            P(None, "tp"),
            P("tp"),
            P("tp"),
            P("tp", None),
            P("tp", None),
            P(),
            P("sp", "tp"),
            P("sp", "tp"),
            P(None, "tp"),
            P(None, "tp"),
            P("tp", None),
            P("tp"),
        ),
        out_specs=P("sp", "tp"),
        check_vma=False,
    )
```

```python
import jax
import jax.numpy as jnp
import numpy as np
from jax import lax
from jax.experimental import pallas as pl
from jax.experimental.pallas import tpu as pltpu
from jax.sharding import PartitionSpec as P

D = 2048
HA = 16
DA = 64
HB = 8
DB = 128
DR = 32
LAT = 256
KC = 3
ROWS = 128
COLS = 256
UNITS = 704
MAIN = 640
HALO = 16
N = 8

THETA = 10000.0
EPS_RMS = 1e-06
EPS_NORM = 1e-05
ALPHA = 2.0**0.25
LOG2E = 1.4426950408889634
LOW = -1e30
MESH = pl.DeviceIdType.MESH
F32 = jnp.float32
BF16 = jnp.bfloat16


def dot(a, b):
    return jnp.dot(a, b, preferred_element_type=F32)


def dot_t(a, b):
    return lax.dot_general(a, b, (((1,), (1,)), ((), ())), preferred_element_type=F32)


class Stages:
    def __init__(self):
        self.scope = None

    def __call__(self, name):
        if self.scope is not None:
            self.scope.__exit__(None, None, None)
        self.scope = None
        if name:
            self.scope = jax.named_scope(name)
            self.scope.__enter__()


def wrap(v):
    return lax.rem(v, N)


def kernel(
    freq_hbm,
    resid_hbm,
    qa_nope_hbm,
    qb_nope_hbm,
    qa_rope_hbm,
    qb_rope_hbm,
    latent_hbm,
    key_rope_hbm,
    lat_gain_hbm,
    wa_key_hbm,
    wa_val_hbm,
    wb_key_hbm,
    wb_val_hbm,
    gain_a_hbm,
    gain_b_hbm,
    wa_out,
    wb_out,
    norm1_gain_hbm,
    ffn_gate_hbm,
    ffn_val_hbm,
    conv_gate_hbm,
    conv_val_hbm,
    ffn_down,
    norm2_gain_hbm,
    out,
    lat,
    wgt,
    q_lat,
    q_rot,
    acc,
    top,
    total,
    w_out,
    w_down,
    mix_out,
    mix_pair,
    mix_in,
    energy,
    pre,
    pre_halo,
    first,
    first_own,
    up,
    hidden,
    down_out,
    down_pair,
    down_in,
    stats,
    local_sem,
    l1s,
    l1r,
    w1s,
    w1r,
    l2s,
    l2r,
    dds,
    ddr,
    xss,
    xsr,
    xds,
    xdr,
    w2s,
    w2r,
    mxs,
    mxr,
    ens,
    enr,
    prs,
    prr,
    hls,
    hlr,
    dns,
    dnr,
    sts,
    srr,
    mps,
    mpr,
    dps,
    dpr,
    input_sem,
    freq,
    resid,
    qa_nope,
    qb_nope,
    qa_rope,
    qb_rope,
    latent,
    key_rope,
    lat_gain,
    wa_key,
    wa_val,
    wb_key,
    wb_val,
    gain_a,
    gain_b,
    norm1_gain,
    ffn_gate,
    ffn_val,
    conv_gate,
    conv_val,
    norm2_gain,
):
    stage = Stages()
    stage("enter")
    sp = lax.axis_index("sp")
    tp = lax.axis_index("tp")
    core = lax.rem(tp, 2)
    z = lax.div(sp, N)
    y = lax.rem(sp, N)
    alpha = y + core * (z - y)
    beta = z + core * (y - z)
    sa = 1 + 7 * core
    sb = 8 - 7 * core
    partner = (sp, tp + 1 - 2 * core)
    sideways = (sp, wrap(tp + 2 + 4 * core))
    parity = lax.rem(lax.div(tp, 2), 2)
    part_of = 2 * parity + core
    nxt = (lax.rem(sp + 1, N * N), tp)
    prv = (lax.rem(sp + N * N - 1, N * N), tp)

    def along_a(k):
        return (wrap(alpha + k) * sa + beta * sb, tp)

    def along_b(k):
        return (alpha * sa + wrap(beta + k) * sb, tp)

    def along_tp(k):
        return (sp, wrap(tp + k))

    def remote(src, dst, send, recv, device):
        return pltpu.make_async_remote_copy(
            src_ref=src, dst_ref=dst, send_sem=send, recv_sem=recv, device_id=device, device_id_type=MESH
        )

    pending = []

    def send(src, dst, ssem, rsem, device):
        copy = remote(src, dst, ssem, rsem, device)
        copy.start()
        pending.append(copy)

    def arrived(ref, rsem):
        remote(ref, ref, l1s.at[0], rsem, partner).wait_recv()

    barrier = pltpu.get_barrier_semaphore()
    peers = [along_a(k) for k in range(1, N)] + [along_b(1), along_b(N - 1)]
    peers += [along_tp(k) for k in range(1, N)]
    peers += [(line[0], t) for line in (nxt, prv) for t in range(N)]
    for device in peers:
        pl.semaphore_signal(barrier, inc=1, device_id=device, device_id_type=MESH)

    local = [
        pltpu.make_async_copy(wa_out, w_out.at[0:128], local_sem.at[0]),
        pltpu.make_async_copy(wb_out, w_out.at[128:256], local_sem.at[1]),
        pltpu.make_async_copy(ffn_down, w_down, local_sem.at[2]),
    ]
    given = [
        (freq_hbm, freq),
        (resid_hbm, resid),
        (qa_nope_hbm, qa_nope),
        (qb_nope_hbm, qb_nope),
        (qa_rope_hbm, qa_rope),
        (qb_rope_hbm, qb_rope),
        (latent_hbm, latent),
        (key_rope_hbm, key_rope),
        (lat_gain_hbm, lat_gain),
        (wa_key_hbm, wa_key),
        (wa_val_hbm, wa_val),
        (wb_key_hbm, wb_key),
        (wb_val_hbm, wb_val),
        (gain_a_hbm, gain_a),
        (gain_b_hbm, gain_b),
        (norm1_gain_hbm, norm1_gain),
        (ffn_gate_hbm, ffn_gate),
        (ffn_val_hbm, ffn_val),
        (conv_gate_hbm, conv_gate),
        (conv_val_hbm, conv_val),
        (norm2_gain_hbm, norm2_gain),
    ]
    entering = [pltpu.make_async_copy(src, dst, input_sem.at[at]) for at, (src, dst) in enumerate(given)]
    for copy in entering + local:
        copy.start()
    for copy in entering:
        copy.wait()

    stage("prep")
    quarter = pl.ds(pl.multiple_of(part_of * 32, 32), 32)
    wide = latent[quarter, :].astype(F32)
    wide = wide * lax.rsqrt(jnp.mean(wide * wide, axis=1, keepdims=True) + EPS_RMS) * lat_gain[...]
    lat_n = wide.astype(BF16)

    spots = sp * ROWS + lax.broadcasted_iota(jnp.int32, (DR // 2, ROWS), 1)
    angle = spots.astype(F32) * freq[...]
    cosine = jnp.cos(angle)
    sine = jnp.sin(angle)

    def rotated(v):
        a = v[: DR // 2].astype(F32)
        b = v[DR // 2 :].astype(F32)
        return jnp.concatenate([a * cosine - b * sine, b * cosine + a * sine], axis=0)

    k_t = rotated(key_rope[...])
    k_packed = jnp.zeros((8, 128), F32)
    for q in range(4):
        taken = [k_t[8 * g : 8 * g + 8, 32 * q : 32 * q + 32] for g in range(4)]
        k_packed = jnp.where(part_of == q, jnp.concatenate(taken, axis=1), k_packed)
    lat[core, beta, alpha, 0:32, :] = lat_n[:, :128]
    lat[core, beta, alpha, 32:64, :] = lat_n[:, 128:]
    lat[core, beta, alpha, 64:80, :] = jnp.concatenate([k_packed, k_packed], axis=0).astype(BF16)
    wgt[beta, alpha, :, 0:MAIN] = ffn_gate[:, :MAIN]
    wgt[beta, alpha, :, MAIN : 2 * MAIN] = ffn_val[:, :MAIN]
    wgt[beta, alpha, :, 2 * MAIN :] = jnp.concatenate(
        [ffn_gate[:, MAIN:].astype(F32), ffn_val[:, MAIN:].astype(F32)], axis=1
    ).astype(BF16)

    stage("barrier")
    pl.semaphore_wait(barrier, len(peers))

    stage("send1")
    mine = lat.at[core, beta, alpha]
    for k in (4, 3, 5, 2, 6, 1, 7):
        send(mine, mine, l1s.at[k - 1], l1r.at[alpha], along_a(k))

    def weight_step(step, forward, backward):
        if forward:
            block = wgt.at[beta, wrap(alpha + N - step)]
            if step:
                arrived(block, w1r.at[wrap(alpha + N - step)])
            send(block, block, w1s.at[step], w1r.at[wrap(alpha + N - step)], along_a(1))
        if backward:
            block = wgt.at[beta, wrap(alpha + step)]
            if step:
                arrived(block, w1r.at[wrap(alpha + step)])
            send(block, block, w1s.at[4 + step], w1r.at[wrap(alpha + step)], along_a(N - 1))

    weight_step(0, True, True)

    stage("queries")
    q_scale_a = (DA + DR) ** (-0.5) * LOG2E
    q_scale_b = (DB + DR) ** (-0.5) * LOG2E
    for h in range(2):
        part = dot_t(qa_nope[:, h * DA : (h + 1) * DA], wa_key[:, h * DA : (h + 1) * DA])
        q_lat[h * ROWS : (h + 1) * ROWS, :] = (part * q_scale_a).astype(BF16)
    part = dot_t(qb_nope[...], wb_key[...])
    q_lat[2 * ROWS :, :] = (part * q_scale_b).astype(BF16)
    turned = [rotated(qa_rope[h * DR : (h + 1) * DR]) * q_scale_a for h in range(2)]
    turned += [rotated(qb_rope[...]) * q_scale_b, jnp.zeros((DR, ROWS), F32)]
    turned = jnp.concatenate(turned, axis=0).T.astype(BF16)
    for h in range(3):
        q_rot[h * ROWS : (h + 1) * ROWS, :] = turned[:, h * DR : (h + 1) * DR]
    acc[...] = jnp.zeros_like(acc)
    top[...] = jnp.full_like(top, LOW)
    total[...] = jnp.zeros_like(total)

    def offset(i):
        steps = lax.div(i + 1, 2)
        return wrap(N + steps * (1 - 2 * lax.rem(i, 2)))

    def lat_piece(b, p):
        return lat.at[core, b, pl.ds(4 * p, 4)]

    def lat_pass(d, p, forward, backward):
        for go, b, k, base in (
            (forward, wrap(beta + N - d), 1, 0),
            (backward, wrap(beta + d), N - 1, 7),
        ):
            if go:
                if d:
                    arrived(lat_piece(b, p), l2r.at[2 * b + p])
                at = base + (2 * d + p if d < 3 else 6)
                send(lat_piece(b, p), lat_piece(b, p), l2s.at[at], l2r.at[2 * b + p], along_b(k))

    def hand_over(b):
        send(lat.at[core, b], lat.at[3 - core, b], xss.at[b], xsr.at[b], sideways)
        send(lat.at[core, b], lat.at[core, b], dds.at[b], ddr.at[b], partner)

    def pass_over(i):
        b = wrap(beta + offset(i))
        block = lat.at[3 - core, b]
        arrived(block, xsr.at[b])
        send(block, block, xds.at[b], xdr.at[b], partner)

    def wgt_piece(b, p):
        pair = lax.rem(lax.div(alpha, 2) + (0, 3, 1, 2)[p], 4)
        return wgt.at[b, pl.ds(2 * pair, 2)]

    def wgt_pass(d, p, forward=True, backward=True):
        for go, b, k, base in (
            (forward, wrap(beta + N - d), 1, 0),
            (backward, wrap(beta + d), N - 1, 14),
        ):
            if go:
                if d:
                    arrived(wgt_piece(b, p), w2r.at[4 * b + p])
                at = base + 4 * d + (p if d < 3 or k == 1 else p - 2)
                send(wgt_piece(b, p), wgt_piece(b, p), w2s.at[at], w2r.at[4 * b + p], along_b(k))

    def attend(*steps):
        stage(f"attend{steps[-1]}")
        places = []
        for i in steps:
            b0 = wrap(z + offset(i))
            b1 = wrap(y + offset(i))
            theirs = wrap(alpha + offset(i))
            arrived(lat.at[1 - core, theirs], ddr.at[theirs])
            arrived(lat.at[2 + core, theirs], xdr.at[theirs])
            places += [(0, b0), (1, b1), (2, b1), (3, b0)]
        rows = lax.broadcasted_iota(jnp.int32, (3 * ROWS, 1), 0)
        rows = sp * ROWS + lax.bitwise_and(rows, ROWS - 1)
        j = lax.broadcasted_iota(jnp.int32, (1, 256), 1)
        a = lax.shift_right_logical(j, 5)
        r = lax.bitwise_and(j, 31)
        old = top[:, 0:1]
        new = old
        keys, scores = [], []
        for slot, b in places:
            left = lat[slot, b, :, 0:32, :].reshape(256, 128)
            right = lat[slot, b, :, 32:64, :].reshape(256, 128)
            keys.append(jnp.concatenate([left, right], axis=1))
            x = lat[slot, b, :, 64:80, :].astype(F32)
            roped = []
            for quad in range(0, N, 4):
                lines = [
                    jnp.concatenate([x[q][0:8, 32 * g : 32 * g + 32] for q in range(quad, quad + 4)], axis=1)
                    for g in range(4)
                ]
                roped.append(jnp.concatenate(lines, axis=0).astype(BF16))
            value = dot_t(q_lat[...], keys[-1]) + dot(q_rot[...], jnp.concatenate(roped, axis=1))
            block = b * N + a if slot in (0, 3) else a * N + b
            which = 2 * parity + slot if slot < 2 else 5 - 2 * parity - slot
            value = jnp.where(block * ROWS + which * 32 + r <= rows, value, LOW)
            new = jnp.maximum(new, jnp.max(value, axis=1, keepdims=True))
            scores.append(value)
        shrink = jnp.exp2(old - new)
        update = acc[...] * shrink
        lanes = total[...] * shrink
        for key, value in zip(keys, scores):
            weights = jnp.exp2(value - new)
            lanes = lanes + (weights[:, :128] + weights[:, 128:])
            update = update + dot(weights.astype(BF16), key)
        acc[...] = update
        total[...] = lanes
        top[...] = jnp.broadcast_to(new, top.shape)

    stage("lat1")
    for k in range(1, N):
        block = lat.at[core, beta, wrap(alpha + k)]
        arrived(block, l1r.at[wrap(alpha + k)])
    stage("ring0")
    lat_pass(0, 0, True, True)
    lat_pass(0, 1, True, True)
    hand_over(beta)
    stage("w1_1")
    weight_step(1, True, True)
    stage("ring1a")
    lat_pass(1, 0, True, True)
    stage("over0")
    pass_over(0)
    stage("ring1b")
    lat_pass(1, 1, True, True)
    hand_over(wrap(beta + N - 1))
    hand_over(wrap(beta + 1))
    stage("w0")
    wgt_pass(0, 0)
    stage("w1_2")
    weight_step(2, True, True)
    stage("ring2a")
    lat_pass(2, 0, True, True)
    stage("over1")
    pass_over(1)
    stage("ring2b")
    lat_pass(2, 1, True, True)
    hand_over(wrap(beta + N - 2))
    hand_over(wrap(beta + 2))
    stage("w1_3")
    weight_step(3, True, False)
    wgt_pass(0, 1)
    attend(0)
    stage("over2")
    pass_over(2)
    attend(1)
    stage("ring3")
    lat_pass(3, 0, True, False)
    lat_pass(3, 1, False, True)
    stage("w1_4")
    for k in (3, 4):
        a = wrap(alpha + k)
        arrived(wgt.at[beta, a], w1r.at[a])
    wgt_pass(0, 2)
    wgt_pass(0, 3)
    stage("p1_0")
    wgt_pass(1, 0)
    stage("ring3end")
    for b, p in ((wrap(beta + N - 3), 1), (wrap(beta + 3), 0)):
        arrived(lat_piece(b, p), l2r.at[2 * b + p])
    hand_over(wrap(beta + N - 3))
    hand_over(wrap(beta + 3))
    stage("over3")
    pass_over(3)
    attend(2)
    stage("ring4")
    b = wrap(beta + 4)
    arrived(lat_piece(b, 0), l2r.at[2 * b])
    arrived(lat_piece(b, 1), l2r.at[2 * b + 1])
    hand_over(wrap(beta + 4))
    stage("over4")
    pass_over(4)
    attend(3)
    stage("p1_1")
    wgt_pass(1, 1)
    stage("over5")
    pass_over(5)
    attend(4)
    stage("p1_2")
    wgt_pass(1, 2)
    stage("over6")
    pass_over(6)
    stage("over7")
    pass_over(7)
    attend(5)
    stage("p1_3")
    wgt_pass(1, 3)
    attend(6, 7)
    stage("p2_0")
    wgt_pass(2, 0)
    stage("p2_1")
    wgt_pass(2, 1)
    stage("heads")
    normed = (acc[...] / jnp.sum(total[...], axis=1, keepdims=True)).astype(BF16)
    raw_a = jnp.concatenate(
        [dot(normed[h * ROWS : (h + 1) * ROWS], wa_val[:, h * DA : (h + 1) * DA]) for h in range(2)], axis=1
    )
    raw_b = dot(normed[2 * ROWS :], wb_val[...])
    power = jnp.sum(raw_a * raw_a, axis=1, keepdims=True) + jnp.sum(raw_b * raw_b, axis=1, keepdims=True)
    energy[4] = jnp.broadcast_to(power, (ROWS, ROWS)).T[0:8]
    gained = jnp.concatenate([raw_a * gain_a[...], raw_b * gain_b[...]], axis=1).astype(BF16)
    local[0].wait()
    local[1].wait()

    def of_tp(t):
        return pl.ds(pl.multiple_of(t * COLS, COLS), COLS)

    chip = lax.div(tp, 2)

    def scattered(partial, leaving, paired, coming, pxs, pxr, ssem, rsem, between):
        for k in (2, 1, 3, 0):
            at = lax.rem(chip + k, 4)
            t = 2 * at + 1 - core
            leaving[t] = partial(t).astype(BF16)
            send(leaving.at[t], paired.at[at], pxs.at[k], pxr.at[at], partner)
        between()
        for k in (2, 1, 3):
            at = lax.rem(chip + k, 4)
            t = 2 * at + core
            value = partial(t)
            arrived(paired.at[at], pxr.at[at])
            leaving[t] = (value + paired[at].astype(F32)).astype(BF16)
            send(leaving.at[t], coming.at[chip], ssem.at[k], rsem.at[chip], (sp, t))
        value = partial(tp)
        arrived(paired.at[chip], pxr.at[chip])
        return value + paired[chip].astype(F32)

    def collected(value, coming, rsem):
        for k in (1, 3, 2):
            at = lax.rem(chip + k, 4)
            arrived(coming.at[at], rsem.at[at])
            value = value + coming[at].astype(F32)
        return value

    def share_energy():
        send(energy.at[4], energy.at[5], ens.at[0], enr.at[4], partner)

    mix = scattered(
        lambda t: dot(gained, w_out[:, of_tp(t)]), mix_out, mix_pair, mix_in, mps, mpr, mxs, mxr, share_energy
    )
    arrived(energy.at[5], enr.at[4])
    energy[chip] = energy[4] + energy[5]
    for k in (2, 1, 3):
        to = (sp, wrap(tp + 2 * k))
        send(energy.at[chip], energy.at[chip], ens.at[k], enr.at[chip], to)
    stage("pass2_23")
    wgt_pass(2, 2)
    wgt_pass(2, 3)
    stage("mixwait")
    mix = collected(mix, mix_in, mxr)
    for k in (1, 2, 3):
        at = lax.rem(chip + k, 4)
        arrived(energy.at[at], enr.at[at])
    stage("mixsum")
    power = energy[0] + energy[1] + energy[2] + energy[3]
    factor = lax.rsqrt(power[0:1] / (HA * DA + HB * DB) + EPS_RMS)
    factor = jnp.broadcast_to(factor, (ROWS, ROWS)).T[:, 0:1]
    pre[tp] = (ALPHA * resid[...].astype(F32) + mix * factor).astype(BF16)
    for k in (4, 2, 6):
        send(pre.at[tp], pre.at[tp], prs.at[k], prr.at[tp], along_tp(k))
    send(pre.at[tp], pre.at[tp], prs.at[1], prr.at[tp], partner)
    for t in range(N):
        send(pre.at[tp, ROWS - HALO : ROWS], pre_halo.at[tp], hls.at[t], hlr.at[tp], (nxt[0], t))
    stage("pass3a")
    wgt_pass(3, 0, True, False)
    wgt_pass(3, 2, False, True)
    wgt_pass(3, 1, True, False)
    stage("prewait")
    center_sum = {}

    def note(t, key):
        value = pre[t].astype(F32)
        amount = jnp.sum(value, axis=1, keepdims=True)
        shifted = value - amount / COLS
        center_sum[key] = (amount, jnp.sum(shifted * shifted, axis=1, keepdims=True))

    note(tp, 0)
    for k in (2, 6, 4):
        t = wrap(tp + k)
        arrived(pre.at[t], prr.at[t])
        send(pre.at[t], pre.at[t], prs.at[k + 1], prr.at[t], partner)
        if k == 2:
            wgt_pass(3, 3, False, True)
        note(t, k)
    stage("halowait")
    for t in range(N):
        arrived(pre_halo.at[t], hlr.at[t])

    def row_stats(ref):
        middle = jnp.sum(ref[0].astype(F32), axis=1, keepdims=True)
        for t in range(1, N):
            middle = middle + jnp.sum(ref[t].astype(F32), axis=1, keepdims=True)
        middle = middle / D
        wide = jnp.zeros_like(middle)
        for t in range(N):
            shifted = ref[t].astype(F32) - middle
            wide = wide + jnp.sum(shifted * shifted, axis=1, keepdims=True)
        return middle, lax.rsqrt(wide / D + EPS_NORM)

    center_halo, scale_halo = row_stats(pre_halo)
    stage("prewait2")
    for k in (1, 3, 7, 5):
        t = tp + 1 - 2 * core if k == 1 else wrap(tp + 1 - 2 * core + k - 1)
        arrived(pre.at[t], prr.at[t])
        note(t, k)

    stage("norm1")
    center = sum(amount for amount, _ in center_sum.values()) / D
    wide = sum(apart for _, apart in center_sum.values())
    for amount, _ in center_sum.values():
        gap = amount / COLS - center
        wide = wide + COLS * gap * gap
    scale = lax.rsqrt(wide / D + EPS_NORM)

    def normed_cols(t):
        gain = norm1_gain[:, t * COLS : (t + 1) * COLS]
        above = (pre_halo[t].astype(F32) - center_halo) * scale_halo * gain
        return jnp.concatenate([above, (pre[t].astype(F32) - center) * scale * gain], axis=0).astype(BF16)

    own = (pre[tp].astype(F32) - center) * scale * norm1_gain[:, of_tp(tp)]
    first_own[...] = own.astype(BF16)

    @pl.when(core == 0)
    def _():
        for t in range(N):
            first[:, t * COLS : (t + 1) * COLS] = normed_cols(t)

    @pl.when(core == 1)
    def _():
        for quad in range(0, N, 4):
            values = [normed_cols(t) for t in range(quad, quad + 4)]
            for g in range(N):
                at = g * COLS + quad * 32
                first[:, at : at + 128] = jnp.concatenate([v[:, g * 32 : g * 32 + 32] for v in values], axis=1)

    def project(i):
        b = wrap(beta + offset(i))
        return dot(first[:, of_tp(b)], wgt[b].reshape(COLS, 2 * UNITS))

    def project_more(begin, end):
        def body(i, carry):
            up[...] += project(i)
            return carry

        lax.fori_loop(begin, end, body, 0)

    stage("up5")
    up[...] = jnp.zeros_like(up)
    project_more(0, 5)
    stage("wait3")
    for b, p in (
        (wrap(beta + N - 3), 2),
        (wrap(beta + N - 3), 3),
        (wrap(beta + 3), 0),
        (wrap(beta + 3), 1),
    ):
        arrived(wgt_piece(b, p), w2r.at[4 * b + p])
    stage("up7")
    project_more(5, 7)
    stage("wait4")
    b = wrap(beta + 4)
    for p in range(4):
        arrived(wgt_piece(b, p), w2r.at[4 * b + p])
    stage("up8")
    project_more(7, 8)

    stage("conv")
    up[...] = up[...].astype(BF16).astype(F32)

    @pl.when(sp == 0)
    def _():
        up[0:HALO, :] = jnp.zeros((HALO, 2 * UNITS), F32)

    def conv(taps, at, width):
        value = taps[0:1] * up[HALO - 2 : HALO - 2 + ROWS, at : at + width]
        value = value + taps[1:2] * up[HALO - 1 : HALO - 1 + ROWS, at : at + width]
        return value + taps[2:3] * up[HALO : HALO + ROWS, at : at + width]

    def gated(g, v):
        return (g / (1.0 + jnp.exp(-g)) * v).astype(BF16)

    for at in range(0, MAIN, 128):
        g = conv(conv_gate[:, at : at + 128], at, 128)
        v = conv(conv_val[:, at : at + 128], MAIN + at, 128)
        hidden[:, at : at + 128] = gated(g, v)
    taps = jnp.concatenate([conv_gate[:, MAIN:], conv_val[:, MAIN:]], axis=1)
    both = conv(taps, 2 * MAIN, 128)
    hidden[:, MAIN:] = gated(both[:, :64], both[:, 64:])

    stage("down")
    local[2].wait()
    value = scattered(
        lambda t: dot(hidden[...], w_down[:, of_tp(t)]), down_out, down_pair, down_in, dps, dpr, dns, dnr, lambda: None
    )
    value = value + ALPHA * first_own[...].astype(F32)
    stage("downwait")
    value = collected(value, down_in, dnr)
    stage("stats")
    amount = jnp.sum(value, axis=1, keepdims=True)
    apart = value - amount / COLS
    apart = jnp.sum(apart * apart, axis=1, keepdims=True)
    line = lax.broadcasted_iota(jnp.int32, (8, ROWS), 0)
    stats[tp] = jnp.where(
        line == 0,
        jnp.broadcast_to(amount, (ROWS, ROWS)).T[0:8],
        jnp.broadcast_to(apart, (ROWS, ROWS)).T[0:8],
    )
    for k in (4, 5, 3, 2, 6, 7, 1):
        send(stats.at[tp], stats.at[tp], sts.at[k], srr.at[tp], along_tp(k))
    stage("statswait")
    for k in range(1, N):
        t = wrap(tp + k)
        arrived(stats.at[t], srr.at[t])
    stage("finish")
    whole = stats[0]
    for t in range(1, N):
        whole = whole + stats[t]
    center = whole[0:1] / D
    spread = whole[1:2]
    for t in range(N):
        gap = stats[t][0:1] / COLS - center
        spread = spread + COLS * gap * gap
    scale = lax.rsqrt(spread / D + EPS_NORM)
    center = jnp.broadcast_to(center, (ROWS, ROWS)).T[:, 0:1]
    scale = jnp.broadcast_to(scale, (ROWS, ROWS)).T[:, 0:1]
    out[...] = ((value - center) * scale * norm2_gain[...]).astype(BF16)

    stage("drain")
    for copy in pending:
        copy.wait_send()
    stage(None)


def shards(*args):
    (
        resid,
        qa_nope,
        qb_nope,
        qa_rope,
        qb_rope,
        latent,
        key_rope,
        lat_gain,
        wa_key,
        wa_val,
        wb_key,
        wb_val,
        gain_a,
        gain_b,
        wa_out,
        wb_out,
        norm1_gain,
        ffn_gate,
        ffn_val,
        conv_gate,
        conv_val,
        ffn_down,
        norm2_gain,
    ) = args
    freq = np.float64(THETA) ** (-np.arange(DR // 2) * 2.0 / DR)
    freq = jnp.asarray(np.broadcast_to(freq[:, None], (DR // 2, ROWS)).astype(np.float32))
    vmem = pl.BlockSpec(memory_space=pltpu.VMEM)
    anywhere = pl.BlockSpec(memory_space=pl.ANY)
    operands = (
        freq,
        resid,
        qa_nope,
        qb_nope,
        qa_rope.T,
        qb_rope.T,
        latent,
        key_rope.T,
        lat_gain[None],
        wa_key,
        wa_val,
        wb_key,
        wb_val,
        gain_a[None],
        gain_b[None],
        wa_out,
        wb_out,
        norm1_gain[None],
        ffn_gate,
        ffn_val,
        conv_gate,
        conv_val,
        ffn_down,
        norm2_gain[None],
    )
    specs = [anywhere] * len(operands)
    small = [x for at, x in enumerate(operands) if at not in (15, 16, 22)]
    dma = pltpu.SemaphoreType.DMA
    return pl.pallas_call(
        kernel,
        out_shape=pltpu.VMEM((ROWS, COLS), BF16),
        in_specs=specs,
        out_specs=vmem,
        scratch_shapes=[
            pltpu.VMEM((4, N, N, 80, 128), BF16),
            pltpu.VMEM((N, N, 32, 2 * UNITS), BF16),
            pltpu.VMEM((3 * ROWS, LAT), BF16),
            pltpu.VMEM((3 * ROWS, DR), BF16),
            pltpu.VMEM((3 * ROWS, LAT), F32),
            pltpu.VMEM((3 * ROWS, 128), F32),
            pltpu.VMEM((3 * ROWS, 128), F32),
            pltpu.VMEM((256, D), BF16),
            pltpu.VMEM((UNITS, D), BF16),
            pltpu.VMEM((N, ROWS, COLS), BF16),
            pltpu.VMEM((4, ROWS, COLS), BF16),
            pltpu.VMEM((4, ROWS, COLS), BF16),
            pltpu.VMEM((N, 8, ROWS), F32),
            pltpu.VMEM((N, ROWS, COLS), BF16),
            pltpu.VMEM((N, HALO, COLS), BF16),
            pltpu.VMEM((HALO + ROWS, D), BF16),
            pltpu.VMEM((ROWS, COLS), BF16),
            pltpu.VMEM((HALO + ROWS, 2 * UNITS), F32),
            pltpu.VMEM((ROWS, UNITS), BF16),
            pltpu.VMEM((N, ROWS, COLS), BF16),
            pltpu.VMEM((4, ROWS, COLS), BF16),
            pltpu.VMEM((4, ROWS, COLS), BF16),
            pltpu.VMEM((N, 8, ROWS), F32),
            dma((3,)),
            dma((7,)),
            dma((8,)),
            dma((8,)),
            dma((8,)),
            dma((14,)),
            dma((16,)),
            dma((8,)),
            dma((8,)),
            dma((8,)),
            dma((8,)),
            dma((8,)),
            dma((8,)),
            dma((28,)),
            dma((32,)),
            dma((8,)),
            dma((8,)),
            dma((8,)),
            dma((8,)),
            dma((8,)),
            dma((8,)),
            dma((8,)),
            dma((8,)),
            dma((8,)),
            dma((8,)),
            dma((8,)),
            dma((8,)),
            dma((4,)),
            dma((4,)),
            dma((4,)),
            dma((4,)),
            dma((len(small),)),
            *[pltpu.VMEM(x.shape, x.dtype) for x in small],
        ],
        compiler_params=pltpu.CompilerParams(
            collective_id=0, has_side_effects=True, vmem_limit_bytes=56 * 1024 * 1024
        ),
        cost_estimate=pl.CostEstimate(flops=8_000_000_000, bytes_accessed=20_000_000, transcendentals=4_000_000),
    )(*operands)


def solution(mesh):
    return jax.shard_map(
        shards,
        mesh=mesh,
        in_specs=(
            P("sp", "tp"),
            P("sp", "tp"),
            P("sp", "tp"),
            P("sp", "tp"),
            P("sp", "tp"),
            P("sp", None),
            P("sp", None),
            P(),
            P(None, "tp"),
            P(None, "tp"),
            P(None, "tp"),
            P(None, "tp"),
            P("tp"),
            P("tp"),
            P("tp", None),
            P("tp", None),
            P(),
            P("sp", "tp"),
            P("sp", "tp"),
            P(None, "tp"),
            P(None, "tp"),
            P("tp", None),
            P("tp"),
        ),
        out_specs=P("sp", "tp"),
        check_vma=False,
    )
```

```python
import jax
import jax.numpy as jnp
import numpy as np
from jax import lax
from jax.experimental import pallas as pl
from jax.experimental.pallas import tpu as pltpu
from jax.sharding import PartitionSpec as P

D = 2048
HA = 16
DA = 64
HB = 8
DB = 128
DR = 32
LAT = 256
KC = 3
ROWS = 128
COLS = 256
UNITS = 704
MAIN = 640
HALO = 16
N = 8

THETA = 10000.0
EPS_RMS = 1e-06
EPS_NORM = 1e-05
ALPHA = 2.0**0.25
LOG2E = 1.4426950408889634
LOW = -1e30
MESH = pl.DeviceIdType.MESH
F32 = jnp.float32
BF16 = jnp.bfloat16


def dot(a, b):
    return jnp.dot(a, b, preferred_element_type=F32)


def dot_t(a, b):
    return lax.dot_general(a, b, (((1,), (1,)), ((), ())), preferred_element_type=F32)


class Stages:
    def __init__(self):
        self.scope = None

    def __call__(self, name):
        if self.scope is not None:
            self.scope.__exit__(None, None, None)
        self.scope = None
        if name:
            self.scope = jax.named_scope(name)
            self.scope.__enter__()


def wrap(v):
    return lax.rem(v, N)


def kernel(
    freq_hbm,
    resid_hbm,
    qa_nope_hbm,
    qb_nope_hbm,
    qa_rope_hbm,
    qb_rope_hbm,
    latent_hbm,
    key_rope_hbm,
    lat_gain_hbm,
    wa_key_hbm,
    wa_val_hbm,
    wb_key_hbm,
    wb_val_hbm,
    gain_a_hbm,
    gain_b_hbm,
    wa_out,
    wb_out,
    norm1_gain_hbm,
    ffn_gate_hbm,
    ffn_val_hbm,
    conv_gate_hbm,
    conv_val_hbm,
    ffn_down,
    norm2_gain_hbm,
    out,
    lat,
    wgt,
    q_lat,
    q_rot,
    acc,
    top,
    total,
    w_out,
    w_down,
    mix_out,
    mix_pair,
    mix_in,
    energy,
    pre,
    pre_halo,
    first,
    first_own,
    up,
    hidden,
    down_out,
    down_pair,
    down_in,
    stats,
    local_sem,
    l1s,
    l1r,
    w1s,
    w1r,
    l2s,
    l2r,
    dds,
    ddr,
    xss,
    xsr,
    xds,
    xdr,
    w2s,
    w2r,
    mxs,
    mxr,
    ens,
    enr,
    prs,
    prr,
    hls,
    hlr,
    dns,
    dnr,
    sts,
    srr,
    mps,
    mpr,
    dps,
    dpr,
    input_sem,
    freq,
    resid,
    qa_nope,
    qb_nope,
    qa_rope,
    qb_rope,
    latent,
    key_rope,
    lat_gain,
    wa_key,
    wa_val,
    wb_key,
    wb_val,
    gain_a,
    gain_b,
    norm1_gain,
    ffn_gate,
    ffn_val,
    conv_gate,
    conv_val,
    norm2_gain,
):
    stage = Stages()
    stage("enter")
    sp = lax.axis_index("sp")
    tp = lax.axis_index("tp")
    core = lax.rem(tp, 2)
    z = lax.div(sp, N)
    y = lax.rem(sp, N)
    alpha = y + core * (z - y)
    beta = z + core * (y - z)
    sa = 1 + 7 * core
    sb = 8 - 7 * core
    partner = (sp, tp + 1 - 2 * core)
    sideways = (sp, wrap(tp + 2 + 4 * core))
    parity = lax.rem(lax.div(tp, 2), 2)
    part_of = 2 * parity + core
    nxt = (lax.rem(sp + 1, N * N), tp)
    prv = (lax.rem(sp + N * N - 1, N * N), tp)

    def along_a(k):
        return (wrap(alpha + k) * sa + beta * sb, tp)

    def along_b(k):
        return (alpha * sa + wrap(beta + k) * sb, tp)

    def along_tp(k):
        return (sp, wrap(tp + k))

    def remote(src, dst, send, recv, device):
        return pltpu.make_async_remote_copy(
            src_ref=src, dst_ref=dst, send_sem=send, recv_sem=recv, device_id=device, device_id_type=MESH
        )

    pending = []

    def send(src, dst, ssem, rsem, device):
        copy = remote(src, dst, ssem, rsem, device)
        copy.start()
        pending.append(copy)

    def arrived(ref, rsem):
        remote(ref, ref, l1s.at[0], rsem, partner).wait_recv()

    barrier = pltpu.get_barrier_semaphore()
    peers = [along_a(k) for k in range(1, N)] + [along_b(1), along_b(N - 1)]
    peers += [along_tp(k) for k in range(1, N)]
    peers += [(line[0], t) for line in (nxt, prv) for t in range(N)]
    for device in peers:
        pl.semaphore_signal(barrier, inc=1, device_id=device, device_id_type=MESH)

    local = [
        pltpu.make_async_copy(wa_out, w_out.at[0:128], local_sem.at[0]),
        pltpu.make_async_copy(wb_out, w_out.at[128:256], local_sem.at[1]),
        pltpu.make_async_copy(ffn_down, w_down, local_sem.at[2]),
    ]
    given = [
        (freq_hbm, freq),
        (resid_hbm, resid),
        (qa_nope_hbm, qa_nope),
        (qb_nope_hbm, qb_nope),
        (qa_rope_hbm, qa_rope),
        (qb_rope_hbm, qb_rope),
        (latent_hbm, latent),
        (key_rope_hbm, key_rope),
        (lat_gain_hbm, lat_gain),
        (wa_key_hbm, wa_key),
        (wa_val_hbm, wa_val),
        (wb_key_hbm, wb_key),
        (wb_val_hbm, wb_val),
        (gain_a_hbm, gain_a),
        (gain_b_hbm, gain_b),
        (norm1_gain_hbm, norm1_gain),
        (ffn_gate_hbm, ffn_gate),
        (ffn_val_hbm, ffn_val),
        (conv_gate_hbm, conv_gate),
        (conv_val_hbm, conv_val),
        (norm2_gain_hbm, norm2_gain),
    ]
    entering = [pltpu.make_async_copy(src, dst, input_sem.at[at]) for at, (src, dst) in enumerate(given)]
    for copy in entering + local:
        copy.start()
    for copy in entering:
        copy.wait()

    stage("prep")
    quarter = pl.ds(pl.multiple_of(part_of * 32, 32), 32)
    wide = latent[quarter, :].astype(F32)
    wide = wide * lax.rsqrt(jnp.mean(wide * wide, axis=1, keepdims=True) + EPS_RMS) * lat_gain[...]
    lat_n = wide.astype(BF16)

    spots = sp * ROWS + lax.broadcasted_iota(jnp.int32, (DR // 2, ROWS), 1)
    angle = spots.astype(F32) * freq[...]
    cosine = jnp.cos(angle)
    sine = jnp.sin(angle)

    def rotated(v):
        a = v[: DR // 2].astype(F32)
        b = v[DR // 2 :].astype(F32)
        return jnp.concatenate([a * cosine - b * sine, b * cosine + a * sine], axis=0)

    k_t = rotated(key_rope[...])
    k_packed = jnp.zeros((8, 128), F32)
    for q in range(4):
        taken = [k_t[8 * g : 8 * g + 8, 32 * q : 32 * q + 32] for g in range(4)]
        k_packed = jnp.where(part_of == q, jnp.concatenate(taken, axis=1), k_packed)
    lat[core, beta, alpha, 0:32, :] = lat_n[:, :128]
    lat[core, beta, alpha, 32:64, :] = lat_n[:, 128:]
    lat[core, beta, alpha, 64:80, :] = jnp.concatenate([k_packed, k_packed], axis=0).astype(BF16)
    wgt[beta, alpha, :, 0:MAIN] = ffn_gate[:, :MAIN]
    wgt[beta, alpha, :, MAIN : 2 * MAIN] = ffn_val[:, :MAIN]
    wgt[beta, alpha, :, 2 * MAIN :] = jnp.concatenate(
        [ffn_gate[:, MAIN:].astype(F32), ffn_val[:, MAIN:].astype(F32)], axis=1
    ).astype(BF16)

    stage("barrier")
    pl.semaphore_wait(barrier, len(peers))

    stage("send1")
    mine = lat.at[core, beta, alpha]
    for k in (4, 3, 5, 2, 6, 1, 7):
        send(mine, mine, l1s.at[k - 1], l1r.at[alpha], along_a(k))

    def weight_step(step, forward, backward):
        if forward:
            block = wgt.at[beta, wrap(alpha + N - step)]
            if step:
                arrived(block, w1r.at[wrap(alpha + N - step)])
            send(block, block, w1s.at[step], w1r.at[wrap(alpha + N - step)], along_a(1))
        if backward:
            block = wgt.at[beta, wrap(alpha + step)]
            if step:
                arrived(block, w1r.at[wrap(alpha + step)])
            send(block, block, w1s.at[4 + step], w1r.at[wrap(alpha + step)], along_a(N - 1))

    weight_step(0, True, True)

    stage("queries")
    q_scale_a = (DA + DR) ** (-0.5) * LOG2E
    q_scale_b = (DB + DR) ** (-0.5) * LOG2E
    for h in range(2):
        part = dot_t(qa_nope[:, h * DA : (h + 1) * DA], wa_key[:, h * DA : (h + 1) * DA])
        q_lat[h * ROWS : (h + 1) * ROWS, :] = (part * q_scale_a).astype(BF16)
    part = dot_t(qb_nope[...], wb_key[...])
    q_lat[2 * ROWS :, :] = (part * q_scale_b).astype(BF16)
    turned = [rotated(qa_rope[h * DR : (h + 1) * DR]) * q_scale_a for h in range(2)]
    turned += [rotated(qb_rope[...]) * q_scale_b, jnp.zeros((DR, ROWS), F32)]
    turned = jnp.concatenate(turned, axis=0).T.astype(BF16)
    for h in range(3):
        q_rot[h * ROWS : (h + 1) * ROWS, :] = turned[:, h * DR : (h + 1) * DR]
    acc[...] = jnp.zeros_like(acc)
    top[...] = jnp.full_like(top, LOW)
    total[...] = jnp.zeros_like(total)

    def offset(i):
        steps = lax.div(i + 1, 2)
        return wrap(N + steps * (1 - 2 * lax.rem(i, 2)))

    def lat_piece(b, p):
        return lat.at[core, b, pl.ds(4 * p, 4)]

    def lat_pass(d, p, forward, backward):
        for go, b, k, base in (
            (forward, wrap(beta + N - d), 1, 0),
            (backward, wrap(beta + d), N - 1, 7),
        ):
            if go:
                if d:
                    arrived(lat_piece(b, p), l2r.at[2 * b + p])
                at = base + (2 * d + p if d < 3 else 6)
                send(lat_piece(b, p), lat_piece(b, p), l2s.at[at], l2r.at[2 * b + p], along_b(k))

    def hand_over(b):
        send(lat.at[core, b], lat.at[3 - core, b], xss.at[b], xsr.at[b], sideways)
        send(lat.at[core, b], lat.at[core, b], dds.at[b], ddr.at[b], partner)

    def pass_over(i):
        b = wrap(beta + offset(i))
        block = lat.at[3 - core, b]
        arrived(block, xsr.at[b])
        send(block, block, xds.at[b], xdr.at[b], partner)

    def wgt_piece(b, p):
        pair = lax.rem(lax.div(alpha, 2) + (0, 3, 1, 2)[p], 4)
        return wgt.at[b, pl.ds(2 * pair, 2)]

    def wgt_pass(d, p, forward=True, backward=True):
        for go, b, k, base in (
            (forward, wrap(beta + N - d), 1, 0),
            (backward, wrap(beta + d), N - 1, 14),
        ):
            if go:
                if d:
                    arrived(wgt_piece(b, p), w2r.at[4 * b + p])
                at = base + 4 * d + (p if d < 3 or k == 1 else p - 2)
                send(wgt_piece(b, p), wgt_piece(b, p), w2s.at[at], w2r.at[4 * b + p], along_b(k))

    def attend(near, *steps):
        stage(f"{'near' if near else 'far'}{steps[-1]}")
        places = []
        for i in steps:
            b0 = wrap(z + offset(i))
            b1 = wrap(y + offset(i))
            theirs = wrap(alpha + offset(i))
            if near:
                arrived(lat.at[1 - core, theirs], ddr.at[theirs])
                places += [(0, b0), (1, b1)]
            else:
                arrived(lat.at[2 + core, theirs], xdr.at[theirs])
                places += [(2, b1), (3, b0)]
        rows = lax.broadcasted_iota(jnp.int32, (3 * ROWS, 1), 0)
        rows = sp * ROWS + lax.bitwise_and(rows, ROWS - 1)
        j = lax.broadcasted_iota(jnp.int32, (1, 256), 1)
        a = lax.shift_right_logical(j, 5)
        r = lax.bitwise_and(j, 31)
        old = top[:, 0:1]
        new = old
        keys, scores = [], []
        for slot, b in places:
            left = lat[slot, b, :, 0:32, :].reshape(256, 128)
            right = lat[slot, b, :, 32:64, :].reshape(256, 128)
            keys.append(jnp.concatenate([left, right], axis=1))
            x = lat[slot, b, :, 64:80, :].astype(F32)
            roped = []
            for quad in range(0, N, 4):
                lines = [
                    jnp.concatenate([x[q][0:8, 32 * g : 32 * g + 32] for q in range(quad, quad + 4)], axis=1)
                    for g in range(4)
                ]
                roped.append(jnp.concatenate(lines, axis=0).astype(BF16))
            value = dot_t(q_lat[...], keys[-1]) + dot(q_rot[...], jnp.concatenate(roped, axis=1))
            block = b * N + a if slot in (0, 3) else a * N + b
            which = 2 * parity + slot if slot < 2 else 5 - 2 * parity - slot
            value = jnp.where(block * ROWS + which * 32 + r <= rows, value, LOW)
            new = jnp.maximum(new, jnp.max(value, axis=1, keepdims=True))
            scores.append(value)
        shrink = jnp.exp2(old - new)
        update = acc[...] * shrink
        lanes = total[...] * shrink
        for key, value in zip(keys, scores):
            weights = jnp.exp2(value - new)
            lanes = lanes + (weights[:, :128] + weights[:, 128:])
            update = update + dot(weights.astype(BF16), key)
        acc[...] = update
        total[...] = lanes
        top[...] = jnp.broadcast_to(new, top.shape)

    stage("lat1")
    for k in range(1, N):
        block = lat.at[core, beta, wrap(alpha + k)]
        arrived(block, l1r.at[wrap(alpha + k)])
    stage("ring0")
    lat_pass(0, 0, True, True)
    lat_pass(0, 1, True, True)
    hand_over(beta)
    stage("w1_1")
    weight_step(1, True, True)
    attend(True, 0)
    stage("ring1a")
    lat_pass(1, 0, True, True)
    stage("over0")
    pass_over(0)
    stage("ring1b")
    lat_pass(1, 1, True, True)
    hand_over(wrap(beta + N - 1))
    hand_over(wrap(beta + 1))
    stage("w0")
    wgt_pass(0, 0)
    stage("w1_2")
    weight_step(2, True, True)
    attend(False, 0)
    stage("ring2a")
    lat_pass(2, 0, True, True)
    stage("over1")
    pass_over(1)
    stage("ring2b")
    lat_pass(2, 1, True, True)
    hand_over(wrap(beta + N - 2))
    hand_over(wrap(beta + 2))
    stage("w1_3")
    weight_step(3, True, False)
    wgt_pass(0, 1)
    attend(True, 1, 2)
    stage("over2")
    pass_over(2)
    stage("ring3")
    lat_pass(3, 0, True, False)
    lat_pass(3, 1, False, True)
    stage("w1_4")
    for k in (3, 4):
        a = wrap(alpha + k)
        arrived(wgt.at[beta, a], w1r.at[a])
    wgt_pass(0, 2)
    wgt_pass(0, 3)
    stage("p1_0")
    wgt_pass(1, 0)
    stage("ring3end")
    for b, p in ((wrap(beta + N - 3), 1), (wrap(beta + 3), 0)):
        arrived(lat_piece(b, p), l2r.at[2 * b + p])
    hand_over(wrap(beta + N - 3))
    hand_over(wrap(beta + 3))
    stage("over3")
    pass_over(3)
    attend(False, 1, 2)
    stage("over4")
    pass_over(4)
    attend(True, 3, 4)
    stage("ring4")
    b = wrap(beta + 4)
    arrived(lat_piece(b, 0), l2r.at[2 * b])
    arrived(lat_piece(b, 1), l2r.at[2 * b + 1])
    hand_over(wrap(beta + 4))
    stage("p1_1")
    wgt_pass(1, 1)
    attend(True, 5, 6)
    stage("over5")
    pass_over(5)
    attend(False, 3, 4)
    stage("p1_2")
    wgt_pass(1, 2)
    stage("over6")
    pass_over(6)
    attend(True, 7)
    stage("p1_3")
    wgt_pass(1, 3)
    stage("over7")
    pass_over(7)
    attend(False, 5, 6)
    stage("p2_0")
    wgt_pass(2, 0)
    attend(False, 7)
    stage("p2_1")
    wgt_pass(2, 1)
    stage("heads")
    normed = (acc[...] / jnp.sum(total[...], axis=1, keepdims=True)).astype(BF16)
    raw_a = jnp.concatenate(
        [dot(normed[h * ROWS : (h + 1) * ROWS], wa_val[:, h * DA : (h + 1) * DA]) for h in range(2)], axis=1
    )
    raw_b = dot(normed[2 * ROWS :], wb_val[...])
    power = jnp.sum(raw_a * raw_a, axis=1, keepdims=True) + jnp.sum(raw_b * raw_b, axis=1, keepdims=True)
    energy[4] = jnp.broadcast_to(power, (ROWS, ROWS)).T[0:8]
    gained = jnp.concatenate([raw_a * gain_a[...], raw_b * gain_b[...]], axis=1).astype(BF16)
    local[0].wait()
    local[1].wait()

    def of_tp(t):
        return pl.ds(pl.multiple_of(t * COLS, COLS), COLS)

    chip = lax.div(tp, 2)

    def scattered(partial, leaving, paired, coming, pxs, pxr, ssem, rsem, between):
        for k in (2, 1, 3, 0):
            at = lax.rem(chip + k, 4)
            t = 2 * at + 1 - core
            leaving[t] = partial(t).astype(BF16)
            send(leaving.at[t], paired.at[at], pxs.at[k], pxr.at[at], partner)
        between()
        for k in (2, 1, 3):
            at = lax.rem(chip + k, 4)
            t = 2 * at + core
            value = partial(t)
            arrived(paired.at[at], pxr.at[at])
            leaving[t] = (value + paired[at].astype(F32)).astype(BF16)
            send(leaving.at[t], coming.at[chip], ssem.at[k], rsem.at[chip], (sp, t))
        value = partial(tp)
        arrived(paired.at[chip], pxr.at[chip])
        return value + paired[chip].astype(F32)

    def collected(value, coming, rsem):
        for k in (1, 3, 2):
            at = lax.rem(chip + k, 4)
            arrived(coming.at[at], rsem.at[at])
            value = value + coming[at].astype(F32)
        return value

    def share_energy():
        send(energy.at[4], energy.at[5], ens.at[0], enr.at[4], partner)

    mix = scattered(
        lambda t: dot(gained, w_out[:, of_tp(t)]), mix_out, mix_pair, mix_in, mps, mpr, mxs, mxr, share_energy
    )
    arrived(energy.at[5], enr.at[4])
    energy[chip] = energy[4] + energy[5]
    for k in (2, 1, 3):
        to = (sp, wrap(tp + 2 * k))
        send(energy.at[chip], energy.at[chip], ens.at[k], enr.at[chip], to)
    stage("pass2_23")
    wgt_pass(2, 2)
    wgt_pass(2, 3)
    stage("mixwait")
    mix = collected(mix, mix_in, mxr)
    for k in (1, 2, 3):
        at = lax.rem(chip + k, 4)
        arrived(energy.at[at], enr.at[at])
    stage("mixsum")
    power = energy[0] + energy[1] + energy[2] + energy[3]
    factor = lax.rsqrt(power[0:1] / (HA * DA + HB * DB) + EPS_RMS)
    factor = jnp.broadcast_to(factor, (ROWS, ROWS)).T[:, 0:1]
    pre[tp] = (ALPHA * resid[...].astype(F32) + mix * factor).astype(BF16)
    for k in (4, 2, 6):
        send(pre.at[tp], pre.at[tp], prs.at[k], prr.at[tp], along_tp(k))
    send(pre.at[tp], pre.at[tp], prs.at[1], prr.at[tp], partner)
    for t in range(N):
        send(pre.at[tp, ROWS - HALO : ROWS], pre_halo.at[tp], hls.at[t], hlr.at[tp], (nxt[0], t))
    stage("pass3a")
    wgt_pass(3, 0, True, False)
    wgt_pass(3, 2, False, True)
    wgt_pass(3, 1, True, False)
    stage("prewait")
    center_sum = {}

    def note(t, key):
        value = pre[t].astype(F32)
        amount = jnp.sum(value, axis=1, keepdims=True)
        shifted = value - amount / COLS
        center_sum[key] = (amount, jnp.sum(shifted * shifted, axis=1, keepdims=True))

    note(tp, 0)
    for k in (2, 6, 4):
        t = wrap(tp + k)
        arrived(pre.at[t], prr.at[t])
        send(pre.at[t], pre.at[t], prs.at[k + 1], prr.at[t], partner)
        if k == 2:
            wgt_pass(3, 3, False, True)
        note(t, k)
    stage("halowait")
    for t in range(N):
        arrived(pre_halo.at[t], hlr.at[t])

    def row_stats(ref):
        middle = jnp.sum(ref[0].astype(F32), axis=1, keepdims=True)
        for t in range(1, N):
            middle = middle + jnp.sum(ref[t].astype(F32), axis=1, keepdims=True)
        middle = middle / D
        wide = jnp.zeros_like(middle)
        for t in range(N):
            shifted = ref[t].astype(F32) - middle
            wide = wide + jnp.sum(shifted * shifted, axis=1, keepdims=True)
        return middle, lax.rsqrt(wide / D + EPS_NORM)

    center_halo, scale_halo = row_stats(pre_halo)
    stage("prewait2")
    for k in (1, 3, 7, 5):
        t = tp + 1 - 2 * core if k == 1 else wrap(tp + 1 - 2 * core + k - 1)
        arrived(pre.at[t], prr.at[t])
        note(t, k)

    stage("norm1")
    center = sum(amount for amount, _ in center_sum.values()) / D
    wide = sum(apart for _, apart in center_sum.values())
    for amount, _ in center_sum.values():
        gap = amount / COLS - center
        wide = wide + COLS * gap * gap
    scale = lax.rsqrt(wide / D + EPS_NORM)

    def normed_cols(t):
        gain = norm1_gain[:, t * COLS : (t + 1) * COLS]
        above = (pre_halo[t].astype(F32) - center_halo) * scale_halo * gain
        return jnp.concatenate([above, (pre[t].astype(F32) - center) * scale * gain], axis=0).astype(BF16)

    own = (pre[tp].astype(F32) - center) * scale * norm1_gain[:, of_tp(tp)]
    first_own[...] = own.astype(BF16)

    @pl.when(core == 0)
    def _():
        for t in range(N):
            first[:, t * COLS : (t + 1) * COLS] = normed_cols(t)

    @pl.when(core == 1)
    def _():
        for quad in range(0, N, 4):
            values = [normed_cols(t) for t in range(quad, quad + 4)]
            for g in range(N):
                at = g * COLS + quad * 32
                first[:, at : at + 128] = jnp.concatenate([v[:, g * 32 : g * 32 + 32] for v in values], axis=1)

    def project(i):
        b = wrap(beta + offset(i))
        return dot(first[:, of_tp(b)], wgt[b].reshape(COLS, 2 * UNITS))

    def project_more(begin, end):
        def body(i, carry):
            up[...] += project(i)
            return carry

        lax.fori_loop(begin, end, body, 0)

    stage("up5")
    up[...] = jnp.zeros_like(up)
    project_more(0, 5)
    stage("wait3")
    for b, p in (
        (wrap(beta + N - 3), 2),
        (wrap(beta + N - 3), 3),
        (wrap(beta + 3), 0),
        (wrap(beta + 3), 1),
    ):
        arrived(wgt_piece(b, p), w2r.at[4 * b + p])
    stage("up7")
    project_more(5, 7)
    stage("wait4")
    b = wrap(beta + 4)
    for p in range(4):
        arrived(wgt_piece(b, p), w2r.at[4 * b + p])
    stage("up8")
    project_more(7, 8)

    stage("conv")
    up[...] = up[...].astype(BF16).astype(F32)

    @pl.when(sp == 0)
    def _():
        up[0:HALO, :] = jnp.zeros((HALO, 2 * UNITS), F32)

    def conv(taps, at, width):
        value = taps[0:1] * up[HALO - 2 : HALO - 2 + ROWS, at : at + width]
        value = value + taps[1:2] * up[HALO - 1 : HALO - 1 + ROWS, at : at + width]
        return value + taps[2:3] * up[HALO : HALO + ROWS, at : at + width]

    def gated(g, v):
        return (g / (1.0 + jnp.exp(-g)) * v).astype(BF16)

    for at in range(0, MAIN, 128):
        g = conv(conv_gate[:, at : at + 128], at, 128)
        v = conv(conv_val[:, at : at + 128], MAIN + at, 128)
        hidden[:, at : at + 128] = gated(g, v)
    taps = jnp.concatenate([conv_gate[:, MAIN:], conv_val[:, MAIN:]], axis=1)
    both = conv(taps, 2 * MAIN, 128)
    hidden[:, MAIN:] = gated(both[:, :64], both[:, 64:])

    stage("down")
    local[2].wait()
    value = scattered(
        lambda t: dot(hidden[...], w_down[:, of_tp(t)]), down_out, down_pair, down_in, dps, dpr, dns, dnr, lambda: None
    )
    value = value + ALPHA * first_own[...].astype(F32)
    stage("downwait")
    value = collected(value, down_in, dnr)
    stage("stats")
    amount = jnp.sum(value, axis=1, keepdims=True)
    apart = value - amount / COLS
    apart = jnp.sum(apart * apart, axis=1, keepdims=True)
    line = lax.broadcasted_iota(jnp.int32, (8, ROWS), 0)
    stats[tp] = jnp.where(
        line == 0,
        jnp.broadcast_to(amount, (ROWS, ROWS)).T[0:8],
        jnp.broadcast_to(apart, (ROWS, ROWS)).T[0:8],
    )
    for k in (4, 5, 3, 2, 6, 7, 1):
        send(stats.at[tp], stats.at[tp], sts.at[k], srr.at[tp], along_tp(k))
    stage("statswait")
    for k in range(1, N):
        t = wrap(tp + k)
        arrived(stats.at[t], srr.at[t])
    stage("finish")
    whole = stats[0]
    for t in range(1, N):
        whole = whole + stats[t]
    center = whole[0:1] / D
    spread = whole[1:2]
    for t in range(N):
        gap = stats[t][0:1] / COLS - center
        spread = spread + COLS * gap * gap
    scale = lax.rsqrt(spread / D + EPS_NORM)
    center = jnp.broadcast_to(center, (ROWS, ROWS)).T[:, 0:1]
    scale = jnp.broadcast_to(scale, (ROWS, ROWS)).T[:, 0:1]
    out[...] = ((value - center) * scale * norm2_gain[...]).astype(BF16)

    stage("drain")
    for copy in pending:
        copy.wait_send()
    stage(None)


def shards(*args):
    (
        resid,
        qa_nope,
        qb_nope,
        qa_rope,
        qb_rope,
        latent,
        key_rope,
        lat_gain,
        wa_key,
        wa_val,
        wb_key,
        wb_val,
        gain_a,
        gain_b,
        wa_out,
        wb_out,
        norm1_gain,
        ffn_gate,
        ffn_val,
        conv_gate,
        conv_val,
        ffn_down,
        norm2_gain,
    ) = args
    freq = np.float64(THETA) ** (-np.arange(DR // 2) * 2.0 / DR)
    freq = jnp.asarray(np.broadcast_to(freq[:, None], (DR // 2, ROWS)).astype(np.float32))
    vmem = pl.BlockSpec(memory_space=pltpu.VMEM)
    anywhere = pl.BlockSpec(memory_space=pl.ANY)
    operands = (
        freq,
        resid,
        qa_nope,
        qb_nope,
        qa_rope.T,
        qb_rope.T,
        latent,
        key_rope.T,
        lat_gain[None],
        wa_key,
        wa_val,
        wb_key,
        wb_val,
        gain_a[None],
        gain_b[None],
        wa_out,
        wb_out,
        norm1_gain[None],
        ffn_gate,
        ffn_val,
        conv_gate,
        conv_val,
        ffn_down,
        norm2_gain[None],
    )
    specs = [anywhere] * len(operands)
    small = [x for at, x in enumerate(operands) if at not in (15, 16, 22)]
    dma = pltpu.SemaphoreType.DMA
    return pl.pallas_call(
        kernel,
        out_shape=pltpu.VMEM((ROWS, COLS), BF16),
        in_specs=specs,
        out_specs=vmem,
        scratch_shapes=[
            pltpu.VMEM((4, N, N, 80, 128), BF16),
            pltpu.VMEM((N, N, 32, 2 * UNITS), BF16),
            pltpu.VMEM((3 * ROWS, LAT), BF16),
            pltpu.VMEM((3 * ROWS, DR), BF16),
            pltpu.VMEM((3 * ROWS, LAT), F32),
            pltpu.VMEM((3 * ROWS, 128), F32),
            pltpu.VMEM((3 * ROWS, 128), F32),
            pltpu.VMEM((256, D), BF16),
            pltpu.VMEM((UNITS, D), BF16),
            pltpu.VMEM((N, ROWS, COLS), BF16),
            pltpu.VMEM((4, ROWS, COLS), BF16),
            pltpu.VMEM((4, ROWS, COLS), BF16),
            pltpu.VMEM((N, 8, ROWS), F32),
            pltpu.VMEM((N, ROWS, COLS), BF16),
            pltpu.VMEM((N, HALO, COLS), BF16),
            pltpu.VMEM((HALO + ROWS, D), BF16),
            pltpu.VMEM((ROWS, COLS), BF16),
            pltpu.VMEM((HALO + ROWS, 2 * UNITS), F32),
            pltpu.VMEM((ROWS, UNITS), BF16),
            pltpu.VMEM((N, ROWS, COLS), BF16),
            pltpu.VMEM((4, ROWS, COLS), BF16),
            pltpu.VMEM((4, ROWS, COLS), BF16),
            pltpu.VMEM((N, 8, ROWS), F32),
            dma((3,)),
            dma((7,)),
            dma((8,)),
            dma((8,)),
            dma((8,)),
            dma((14,)),
            dma((16,)),
            dma((8,)),
            dma((8,)),
            dma((8,)),
            dma((8,)),
            dma((8,)),
            dma((8,)),
            dma((28,)),
            dma((32,)),
            dma((8,)),
            dma((8,)),
            dma((8,)),
            dma((8,)),
            dma((8,)),
            dma((8,)),
            dma((8,)),
            dma((8,)),
            dma((8,)),
            dma((8,)),
            dma((8,)),
            dma((8,)),
            dma((4,)),
            dma((4,)),
            dma((4,)),
            dma((4,)),
            dma((len(small),)),
            *[pltpu.VMEM(x.shape, x.dtype) for x in small],
        ],
        compiler_params=pltpu.CompilerParams(
            collective_id=0, has_side_effects=True, vmem_limit_bytes=56 * 1024 * 1024
        ),
        cost_estimate=pl.CostEstimate(flops=8_000_000_000, bytes_accessed=20_000_000, transcendentals=4_000_000),
    )(*operands)


def solution(mesh):
    return jax.shard_map(
        shards,
        mesh=mesh,
        in_specs=(
            P("sp", "tp"),
            P("sp", "tp"),
            P("sp", "tp"),
            P("sp", "tp"),
            P("sp", "tp"),
            P("sp", None),
            P("sp", None),
            P(),
            P(None, "tp"),
            P(None, "tp"),
            P(None, "tp"),
            P(None, "tp"),
            P("tp"),
            P("tp"),
            P("tp", None),
            P("tp", None),
            P(),
            P("sp", "tp"),
            P("sp", "tp"),
            P(None, "tp"),
            P(None, "tp"),
            P("tp", None),
            P("tp"),
        ),
        out_specs=P("sp", "tp"),
        check_vma=False,
    )
```

```python
import jax
import jax.numpy as jnp
import numpy as np
from jax import lax
from jax.experimental import pallas as pl
from jax.experimental.pallas import tpu as pltpu
from jax.sharding import PartitionSpec as P

D = 2048
HA = 16
DA = 64
HB = 8
DB = 128
DR = 32
LAT = 256
KC = 3
ROWS = 128
COLS = 256
UNITS = 704
MAIN = 640
HALO = 16
N = 8

THETA = 10000.0
EPS_RMS = 1e-06
EPS_NORM = 1e-05
ALPHA = 2.0**0.25
LOG2E = 1.4426950408889634
LOW = -1e30
MESH = pl.DeviceIdType.MESH
F32 = jnp.float32
BF16 = jnp.bfloat16


def dot(a, b):
    return jnp.dot(a, b, preferred_element_type=F32)


def dot_t(a, b):
    return lax.dot_general(a, b, (((1,), (1,)), ((), ())), preferred_element_type=F32)


class Stages:
    def __init__(self):
        self.scope = None

    def __call__(self, name):
        if self.scope is not None:
            self.scope.__exit__(None, None, None)
        self.scope = None
        if name:
            self.scope = jax.named_scope(name)
            self.scope.__enter__()


def wrap(v):
    return lax.rem(v, N)


def kernel(
    freq_hbm,
    resid_hbm,
    qa_nope_hbm,
    qb_nope_hbm,
    qa_rope_hbm,
    qb_rope_hbm,
    latent_hbm,
    key_rope_hbm,
    lat_gain_hbm,
    wa_key_hbm,
    wa_val_hbm,
    wb_key_hbm,
    wb_val_hbm,
    gain_a_hbm,
    gain_b_hbm,
    wa_out,
    wb_out,
    norm1_gain_hbm,
    ffn_gate_hbm,
    ffn_val_hbm,
    conv_gate_hbm,
    conv_val_hbm,
    ffn_down,
    norm2_gain_hbm,
    out,
    lat,
    wgt,
    q_lat,
    q_rot,
    acc,
    top,
    total,
    w_out,
    w_down,
    mix_out,
    mix_pair,
    mix_in,
    energy,
    pre,
    pre_halo,
    first,
    first_own,
    up,
    hidden,
    down_out,
    down_pair,
    down_in,
    stats,
    local_sem,
    l1s,
    l1r,
    w1s,
    w1r,
    l2s,
    l2r,
    dds,
    ddr,
    xss,
    xsr,
    xds,
    xdr,
    w2s,
    w2r,
    mxs,
    mxr,
    ens,
    enr,
    prs,
    prr,
    hls,
    hlr,
    dns,
    dnr,
    sts,
    srr,
    mps,
    mpr,
    dps,
    dpr,
    input_sem,
    freq,
    resid,
    qa_nope,
    qb_nope,
    qa_rope,
    qb_rope,
    latent,
    key_rope,
    lat_gain,
    wa_key,
    wa_val,
    wb_key,
    wb_val,
    gain_a,
    gain_b,
    norm1_gain,
    ffn_gate,
    ffn_val,
    conv_gate,
    conv_val,
    norm2_gain,
):
    stage = Stages()
    stage("enter")
    sp = lax.axis_index("sp")
    tp = lax.axis_index("tp")
    core = lax.rem(tp, 2)
    z = lax.div(sp, N)
    y = lax.rem(sp, N)
    alpha = y + core * (z - y)
    beta = z + core * (y - z)
    sa = 1 + 7 * core
    sb = 8 - 7 * core
    partner = (sp, tp + 1 - 2 * core)
    sideways = (sp, wrap(tp + 2 + 4 * core))
    parity = lax.rem(lax.div(tp, 2), 2)
    part_of = 2 * parity + core
    nxt = (lax.rem(sp + 1, N * N), tp)
    prv = (lax.rem(sp + N * N - 1, N * N), tp)

    def along_a(k):
        return (wrap(alpha + k) * sa + beta * sb, tp)

    def along_b(k):
        return (alpha * sa + wrap(beta + k) * sb, tp)

    def along_tp(k):
        return (sp, wrap(tp + k))

    def remote(src, dst, send, recv, device):
        return pltpu.make_async_remote_copy(
            src_ref=src, dst_ref=dst, send_sem=send, recv_sem=recv, device_id=device, device_id_type=MESH
        )

    pending = []

    def send(src, dst, ssem, rsem, device):
        copy = remote(src, dst, ssem, rsem, device)
        copy.start()
        pending.append(copy)

    def arrived(ref, rsem):
        remote(ref, ref, l1s.at[0], rsem, partner).wait_recv()

    barrier = pltpu.get_barrier_semaphore()
    peers = [along_a(k) for k in range(1, N)] + [along_b(1), along_b(N - 1)]
    peers += [along_tp(k) for k in range(1, N)]
    peers += [(line[0], t) for line in (nxt, prv) for t in range(N)]
    for device in peers:
        pl.semaphore_signal(barrier, inc=1, device_id=device, device_id_type=MESH)

    local = [
        pltpu.make_async_copy(wa_out, w_out.at[0:128], local_sem.at[0]),
        pltpu.make_async_copy(wb_out, w_out.at[128:256], local_sem.at[1]),
        pltpu.make_async_copy(ffn_down, w_down, local_sem.at[2]),
    ]
    given = [
        (freq_hbm, freq),
        (resid_hbm, resid),
        (qa_nope_hbm, qa_nope),
        (qb_nope_hbm, qb_nope),
        (qa_rope_hbm, qa_rope),
        (qb_rope_hbm, qb_rope),
        (latent_hbm, latent),
        (key_rope_hbm, key_rope),
        (lat_gain_hbm, lat_gain),
        (wa_key_hbm, wa_key),
        (wa_val_hbm, wa_val),
        (wb_key_hbm, wb_key),
        (wb_val_hbm, wb_val),
        (gain_a_hbm, gain_a),
        (gain_b_hbm, gain_b),
        (norm1_gain_hbm, norm1_gain),
        (ffn_gate_hbm, ffn_gate),
        (ffn_val_hbm, ffn_val),
        (conv_gate_hbm, conv_gate),
        (conv_val_hbm, conv_val),
        (norm2_gain_hbm, norm2_gain),
    ]
    entering = [pltpu.make_async_copy(src, dst, input_sem.at[at]) for at, (src, dst) in enumerate(given)]
    for copy in entering + local:
        copy.start()
    for copy in entering:
        copy.wait()

    stage("prep")
    quarter = pl.ds(pl.multiple_of(part_of * 32, 32), 32)
    wide = latent[quarter, :].astype(F32)
    wide = wide * lax.rsqrt(jnp.mean(wide * wide, axis=1, keepdims=True) + EPS_RMS) * lat_gain[...]
    lat_n = wide.astype(BF16)

    spots = sp * ROWS + lax.broadcasted_iota(jnp.int32, (DR // 2, ROWS), 1)
    angle = spots.astype(F32) * freq[...]
    cosine = jnp.cos(angle)
    sine = jnp.sin(angle)

    def rotated(v):
        a = v[: DR // 2].astype(F32)
        b = v[DR // 2 :].astype(F32)
        return jnp.concatenate([a * cosine - b * sine, b * cosine + a * sine], axis=0)

    k_t = rotated(key_rope[...])
    k_packed = jnp.zeros((8, 128), F32)
    for q in range(4):
        taken = [k_t[8 * g : 8 * g + 8, 32 * q : 32 * q + 32] for g in range(4)]
        k_packed = jnp.where(part_of == q, jnp.concatenate(taken, axis=1), k_packed)
    lat[core, beta, alpha, 0:32, :] = lat_n[:, :128]
    lat[core, beta, alpha, 32:64, :] = lat_n[:, 128:]
    lat[core, beta, alpha, 64:80, :] = jnp.concatenate([k_packed, k_packed], axis=0).astype(BF16)
    wgt[beta, alpha, :, 0:MAIN] = ffn_gate[:, :MAIN]
    wgt[beta, alpha, :, MAIN : 2 * MAIN] = ffn_val[:, :MAIN]
    wgt[beta, alpha, :, 2 * MAIN :] = jnp.concatenate(
        [ffn_gate[:, MAIN:].astype(F32), ffn_val[:, MAIN:].astype(F32)], axis=1
    ).astype(BF16)

    stage("barrier")
    pl.semaphore_wait(barrier, len(peers))

    stage("send1")
    mine = lat.at[core, beta, alpha]
    for k in (4, 3, 5, 2, 6, 1, 7):
        send(mine, mine, l1s.at[k - 1], l1r.at[alpha], along_a(k))

    def weight_step(step, forward, backward):
        if forward:
            block = wgt.at[beta, wrap(alpha + N - step)]
            if step:
                arrived(block, w1r.at[wrap(alpha + N - step)])
            send(block, block, w1s.at[step], w1r.at[wrap(alpha + N - step)], along_a(1))
        if backward:
            block = wgt.at[beta, wrap(alpha + step)]
            if step:
                arrived(block, w1r.at[wrap(alpha + step)])
            send(block, block, w1s.at[4 + step], w1r.at[wrap(alpha + step)], along_a(N - 1))

    weight_step(0, True, True)

    stage("queries")
    q_scale_a = (DA + DR) ** (-0.5) * LOG2E
    q_scale_b = (DB + DR) ** (-0.5) * LOG2E
    for h in range(2):
        part = dot_t(qa_nope[:, h * DA : (h + 1) * DA], wa_key[:, h * DA : (h + 1) * DA])
        q_lat[h * ROWS : (h + 1) * ROWS, :] = (part * q_scale_a).astype(BF16)
    part = dot_t(qb_nope[...], wb_key[...])
    q_lat[2 * ROWS :, :] = (part * q_scale_b).astype(BF16)
    turned = [rotated(qa_rope[h * DR : (h + 1) * DR]) * q_scale_a for h in range(2)]
    turned += [rotated(qb_rope[...]) * q_scale_b, jnp.zeros((DR, ROWS), F32)]
    turned = jnp.concatenate(turned, axis=0).T.astype(BF16)
    for h in range(3):
        q_rot[h * ROWS : (h + 1) * ROWS, :] = turned[:, h * DR : (h + 1) * DR]
    acc[...] = jnp.zeros_like(acc)
    top[...] = jnp.full_like(top, LOW)
    total[...] = jnp.zeros_like(total)

    def offset(i):
        steps = lax.div(i + 1, 2)
        return wrap(N + steps * (1 - 2 * lax.rem(i, 2)))

    def lat_piece(b, p):
        return lat.at[core, b, pl.ds(4 * p, 4)]

    def lat_pass(d, p, forward, backward):
        for go, b, k, base in (
            (forward, wrap(beta + N - d), 1, 0),
            (backward, wrap(beta + d), N - 1, 7),
        ):
            if go:
                if d:
                    arrived(lat_piece(b, p), l2r.at[2 * b + p])
                at = base + (2 * d + p if d < 3 else 6)
                send(lat_piece(b, p), lat_piece(b, p), l2s.at[at], l2r.at[2 * b + p], along_b(k))

    def hand_over(b):
        send(lat.at[core, b], lat.at[3 - core, b], xss.at[b], xsr.at[b], sideways)
        send(lat.at[core, b], lat.at[core, b], dds.at[b], ddr.at[b], partner)

    def pass_over(i):
        b = wrap(beta + offset(i))
        block = lat.at[3 - core, b]
        arrived(block, xsr.at[b])
        send(block, block, xds.at[b], xdr.at[b], partner)

    def wgt_piece(b, p):
        pair = lax.rem(lax.div(alpha, 2) + (0, 3, 1, 2)[p], 4)
        return wgt.at[b, pl.ds(2 * pair, 2)]

    def wgt_pass(d, p, forward=True, backward=True):
        for go, b, k, base in (
            (forward, wrap(beta + N - d), 1, 0),
            (backward, wrap(beta + d), N - 1, 14),
        ):
            if go:
                if d:
                    arrived(wgt_piece(b, p), w2r.at[4 * b + p])
                at = base + 4 * d + (p if d < 3 or k == 1 else p - 2)
                send(wgt_piece(b, p), wgt_piece(b, p), w2s.at[at], w2r.at[4 * b + p], along_b(k))

    def attend(near, *steps):
        stage(f"{'near' if near else 'far'}{steps[-1]}")
        places = []
        for i in steps:
            b0 = wrap(z + offset(i))
            b1 = wrap(y + offset(i))
            theirs = wrap(alpha + offset(i))
            if near:
                arrived(lat.at[1 - core, theirs], ddr.at[theirs])
                places += [(0, b0), (1, b1)]
            else:
                arrived(lat.at[2 + core, theirs], xdr.at[theirs])
                places += [(2, b1), (3, b0)]
        rows = lax.broadcasted_iota(jnp.int32, (3 * ROWS, 1), 0)
        rows = sp * ROWS + lax.bitwise_and(rows, ROWS - 1)
        j = lax.broadcasted_iota(jnp.int32, (1, 256), 1)
        a = lax.shift_right_logical(j, 5)
        r = lax.bitwise_and(j, 31)
        old = top[:, 0:1]
        new = old
        keys, scores = [], []
        for slot, b in places:
            left = lat[slot, b, :, 0:32, :].reshape(256, 128)
            right = lat[slot, b, :, 32:64, :].reshape(256, 128)
            keys.append(jnp.concatenate([left, right], axis=1))
            x = lat[slot, b, :, 64:80, :].astype(F32)
            roped = []
            for quad in range(0, N, 4):
                lines = [
                    jnp.concatenate([x[q][0:8, 32 * g : 32 * g + 32] for q in range(quad, quad + 4)], axis=1)
                    for g in range(4)
                ]
                roped.append(jnp.concatenate(lines, axis=0).astype(BF16))
            value = dot_t(q_lat[...], keys[-1]) + dot(q_rot[...], jnp.concatenate(roped, axis=1))
            block = b * N + a if slot in (0, 3) else a * N + b
            which = 2 * parity + slot if slot < 2 else 5 - 2 * parity - slot
            value = jnp.where(block * ROWS + which * 32 + r <= rows, value, LOW)
            new = jnp.maximum(new, jnp.max(value, axis=1, keepdims=True))
            scores.append(value)
        shrink = jnp.exp2(old - new)
        update = acc[...] * shrink
        lanes = total[...] * shrink
        for key, value in zip(keys, scores):
            weights = jnp.exp2(value - new)
            lanes = lanes + (weights[:, :128] + weights[:, 128:])
            update = update + dot(weights.astype(BF16), key)
        acc[...] = update
        total[...] = lanes
        top[...] = jnp.broadcast_to(new, top.shape)

    stage("lat1")
    for k in range(1, N):
        block = lat.at[core, beta, wrap(alpha + k)]
        arrived(block, l1r.at[wrap(alpha + k)])
    stage("ring0")
    lat_pass(0, 0, True, True)
    lat_pass(0, 1, True, True)
    hand_over(beta)
    stage("w1_1")
    weight_step(1, True, True)
    attend(True, 0)
    stage("ring1a")
    lat_pass(1, 0, True, True)
    stage("over0")
    pass_over(0)
    stage("ring1b")
    lat_pass(1, 1, True, True)
    hand_over(wrap(beta + N - 1))
    hand_over(wrap(beta + 1))
    stage("w0")
    wgt_pass(0, 0)
    stage("w1_2")
    weight_step(2, True, True)
    attend(False, 0)
    stage("ring2a")
    lat_pass(2, 0, True, True)
    stage("over1")
    pass_over(1)
    stage("ring2b")
    lat_pass(2, 1, True, True)
    hand_over(wrap(beta + N - 2))
    hand_over(wrap(beta + 2))
    stage("w1_3")
    weight_step(3, True, False)
    wgt_pass(0, 1)
    attend(True, 1, 2)
    stage("over2")
    pass_over(2)
    stage("ring3")
    lat_pass(3, 0, True, False)
    lat_pass(3, 1, False, True)
    stage("w1_4")
    arrived(wgt.at[beta, wrap(alpha + 3)], w1r.at[wrap(alpha + 3)])
    wgt_pass(0, 2)
    stage("p1_0")
    wgt_pass(1, 0)
    stage("ring3end")
    for b, p in ((wrap(beta + N - 3), 1), (wrap(beta + 3), 0)):
        arrived(lat_piece(b, p), l2r.at[2 * b + p])
    hand_over(wrap(beta + N - 3))
    hand_over(wrap(beta + 3))
    stage("over3")
    pass_over(3)
    stage("w1_5")
    arrived(wgt.at[beta, wrap(alpha + 4)], w1r.at[wrap(alpha + 4)])
    wgt_pass(0, 3)
    attend(False, 1, 2)
    stage("over4")
    pass_over(4)
    attend(True, 3, 4)
    stage("ring4")
    b = wrap(beta + 4)
    arrived(lat_piece(b, 0), l2r.at[2 * b])
    arrived(lat_piece(b, 1), l2r.at[2 * b + 1])
    hand_over(wrap(beta + 4))
    stage("p1_1")
    wgt_pass(1, 1)
    attend(True, 5, 6)
    stage("over5")
    pass_over(5)
    attend(False, 3, 4)
    stage("p1_2")
    wgt_pass(1, 2)
    stage("over6")
    pass_over(6)
    attend(True, 7)
    stage("p1_3")
    wgt_pass(1, 3)
    stage("over7")
    pass_over(7)
    attend(False, 5, 6)
    stage("p2_0")
    wgt_pass(2, 0)
    attend(False, 7)
    stage("p2_1")
    wgt_pass(2, 1)
    stage("heads")
    normed = (acc[...] / jnp.sum(total[...], axis=1, keepdims=True)).astype(BF16)
    raw_a = jnp.concatenate(
        [dot(normed[h * ROWS : (h + 1) * ROWS], wa_val[:, h * DA : (h + 1) * DA]) for h in range(2)], axis=1
    )
    raw_b = dot(normed[2 * ROWS :], wb_val[...])
    power = jnp.sum(raw_a * raw_a, axis=1, keepdims=True) + jnp.sum(raw_b * raw_b, axis=1, keepdims=True)
    energy[4] = jnp.broadcast_to(power, (ROWS, ROWS)).T[0:8]
    gained = jnp.concatenate([raw_a * gain_a[...], raw_b * gain_b[...]], axis=1).astype(BF16)
    local[0].wait()
    local[1].wait()

    def of_tp(t):
        return pl.ds(pl.multiple_of(t * COLS, COLS), COLS)

    chip = lax.div(tp, 2)

    def scattered(partial, leaving, paired, coming, pxs, pxr, ssem, rsem, between):
        for k in (2, 1, 3, 0):
            at = lax.rem(chip + k, 4)
            t = 2 * at + 1 - core
            leaving[t] = partial(t).astype(BF16)
            send(leaving.at[t], paired.at[at], pxs.at[k], pxr.at[at], partner)
        between()
        for k in (2, 1, 3):
            at = lax.rem(chip + k, 4)
            t = 2 * at + core
            value = partial(t)
            arrived(paired.at[at], pxr.at[at])
            leaving[t] = (value + paired[at].astype(F32)).astype(BF16)
            send(leaving.at[t], coming.at[chip], ssem.at[k], rsem.at[chip], (sp, t))
        value = partial(tp)
        arrived(paired.at[chip], pxr.at[chip])
        return value + paired[chip].astype(F32)

    def collected(value, coming, rsem):
        for k in (1, 3, 2):
            at = lax.rem(chip + k, 4)
            arrived(coming.at[at], rsem.at[at])
            value = value + coming[at].astype(F32)
        return value

    def share_energy():
        send(energy.at[4], energy.at[5], ens.at[0], enr.at[4], partner)

    mix = scattered(
        lambda t: dot(gained, w_out[:, of_tp(t)]), mix_out, mix_pair, mix_in, mps, mpr, mxs, mxr, share_energy
    )
    arrived(energy.at[5], enr.at[4])
    energy[chip] = energy[4] + energy[5]
    for k in (2, 1, 3):
        to = (sp, wrap(tp + 2 * k))
        send(energy.at[chip], energy.at[chip], ens.at[k], enr.at[chip], to)
    stage("pass2_23")
    wgt_pass(2, 2)
    wgt_pass(2, 3)
    stage("mixwait")
    mix = collected(mix, mix_in, mxr)
    for k in (1, 2, 3):
        at = lax.rem(chip + k, 4)
        arrived(energy.at[at], enr.at[at])
    stage("mixsum")
    power = energy[0] + energy[1] + energy[2] + energy[3]
    factor = lax.rsqrt(power[0:1] / (HA * DA + HB * DB) + EPS_RMS)
    factor = jnp.broadcast_to(factor, (ROWS, ROWS)).T[:, 0:1]
    pre[tp] = (ALPHA * resid[...].astype(F32) + mix * factor).astype(BF16)
    for k in (4, 2, 6):
        send(pre.at[tp], pre.at[tp], prs.at[k], prr.at[tp], along_tp(k))
    send(pre.at[tp], pre.at[tp], prs.at[1], prr.at[tp], partner)
    for t in range(N):
        send(pre.at[tp, ROWS - HALO : ROWS], pre_halo.at[tp], hls.at[t], hlr.at[tp], (nxt[0], t))
    stage("pass3a")
    wgt_pass(3, 0, True, False)
    wgt_pass(3, 2, False, True)
    wgt_pass(3, 1, True, False)
    stage("prewait")
    center_sum = {}

    def note(t, key):
        value = pre[t].astype(F32)
        amount = jnp.sum(value, axis=1, keepdims=True)
        shifted = value - amount / COLS
        center_sum[key] = (amount, jnp.sum(shifted * shifted, axis=1, keepdims=True))

    note(tp, 0)
    for k in (2, 6, 4):
        t = wrap(tp + k)
        arrived(pre.at[t], prr.at[t])
        send(pre.at[t], pre.at[t], prs.at[k + 1], prr.at[t], partner)
        if k == 2:
            wgt_pass(3, 3, False, True)
        note(t, k)
    stage("halowait")
    for t in range(N):
        arrived(pre_halo.at[t], hlr.at[t])

    def row_stats(ref):
        middle = jnp.sum(ref[0].astype(F32), axis=1, keepdims=True)
        for t in range(1, N):
            middle = middle + jnp.sum(ref[t].astype(F32), axis=1, keepdims=True)
        middle = middle / D
        wide = jnp.zeros_like(middle)
        for t in range(N):
            shifted = ref[t].astype(F32) - middle
            wide = wide + jnp.sum(shifted * shifted, axis=1, keepdims=True)
        return middle, lax.rsqrt(wide / D + EPS_NORM)

    center_halo, scale_halo = row_stats(pre_halo)
    stage("prewait2")
    for k in (1, 3, 7, 5):
        t = tp + 1 - 2 * core if k == 1 else wrap(tp + 1 - 2 * core + k - 1)
        arrived(pre.at[t], prr.at[t])
        note(t, k)

    stage("norm1")
    center = sum(amount for amount, _ in center_sum.values()) / D
    wide = sum(apart for _, apart in center_sum.values())
    for amount, _ in center_sum.values():
        gap = amount / COLS - center
        wide = wide + COLS * gap * gap
    scale = lax.rsqrt(wide / D + EPS_NORM)

    def normed_cols(t):
        gain = norm1_gain[:, t * COLS : (t + 1) * COLS]
        above = (pre_halo[t].astype(F32) - center_halo) * scale_halo * gain
        return jnp.concatenate([above, (pre[t].astype(F32) - center) * scale * gain], axis=0).astype(BF16)

    own = (pre[tp].astype(F32) - center) * scale * norm1_gain[:, of_tp(tp)]
    first_own[...] = own.astype(BF16)

    @pl.when(core == 0)
    def _():
        for t in range(N):
            first[:, t * COLS : (t + 1) * COLS] = normed_cols(t)

    @pl.when(core == 1)
    def _():
        for quad in range(0, N, 4):
            values = [normed_cols(t) for t in range(quad, quad + 4)]
            for g in range(N):
                at = g * COLS + quad * 32
                first[:, at : at + 128] = jnp.concatenate([v[:, g * 32 : g * 32 + 32] for v in values], axis=1)

    def project(i):
        b = wrap(beta + offset(i))
        return dot(first[:, of_tp(b)], wgt[b].reshape(COLS, 2 * UNITS))

    def project_more(begin, end):
        def body(i, carry):
            up[...] += project(i)
            return carry

        lax.fori_loop(begin, end, body, 0)

    stage("up5")
    up[...] = jnp.zeros_like(up)
    project_more(0, 5)
    stage("wait3")
    for b, p in (
        (wrap(beta + N - 3), 2),
        (wrap(beta + N - 3), 3),
        (wrap(beta + 3), 0),
        (wrap(beta + 3), 1),
    ):
        arrived(wgt_piece(b, p), w2r.at[4 * b + p])
    stage("up7")
    project_more(5, 7)
    stage("wait4")
    b = wrap(beta + 4)
    for p in range(4):
        arrived(wgt_piece(b, p), w2r.at[4 * b + p])
    stage("up8")
    project_more(7, 8)

    stage("conv")
    up[...] = up[...].astype(BF16).astype(F32)

    @pl.when(sp == 0)
    def _():
        up[0:HALO, :] = jnp.zeros((HALO, 2 * UNITS), F32)

    def conv(taps, at, width):
        value = taps[0:1] * up[HALO - 2 : HALO - 2 + ROWS, at : at + width]
        value = value + taps[1:2] * up[HALO - 1 : HALO - 1 + ROWS, at : at + width]
        return value + taps[2:3] * up[HALO : HALO + ROWS, at : at + width]

    def gated(g, v):
        return (g / (1.0 + jnp.exp(-g)) * v).astype(BF16)

    for at in range(0, MAIN, 128):
        g = conv(conv_gate[:, at : at + 128], at, 128)
        v = conv(conv_val[:, at : at + 128], MAIN + at, 128)
        hidden[:, at : at + 128] = gated(g, v)
    taps = jnp.concatenate([conv_gate[:, MAIN:], conv_val[:, MAIN:]], axis=1)
    both = conv(taps, 2 * MAIN, 128)
    hidden[:, MAIN:] = gated(both[:, :64], both[:, 64:])

    stage("down")
    local[2].wait()
    value = scattered(
        lambda t: dot(hidden[...], w_down[:, of_tp(t)]), down_out, down_pair, down_in, dps, dpr, dns, dnr, lambda: None
    )
    value = value + ALPHA * first_own[...].astype(F32)
    stage("downwait")
    value = collected(value, down_in, dnr)
    stage("stats")
    amount = jnp.sum(value, axis=1, keepdims=True)
    apart = value - amount / COLS
    apart = jnp.sum(apart * apart, axis=1, keepdims=True)
    line = lax.broadcasted_iota(jnp.int32, (8, ROWS), 0)
    stats[tp] = jnp.where(
        line == 0,
        jnp.broadcast_to(amount, (ROWS, ROWS)).T[0:8],
        jnp.broadcast_to(apart, (ROWS, ROWS)).T[0:8],
    )
    for k in (4, 5, 3, 2, 6, 7, 1):
        send(stats.at[tp], stats.at[tp], sts.at[k], srr.at[tp], along_tp(k))
    stage("statswait")
    for k in range(1, N):
        t = wrap(tp + k)
        arrived(stats.at[t], srr.at[t])
    stage("finish")
    whole = stats[0]
    for t in range(1, N):
        whole = whole + stats[t]
    center = whole[0:1] / D
    spread = whole[1:2]
    for t in range(N):
        gap = stats[t][0:1] / COLS - center
        spread = spread + COLS * gap * gap
    scale = lax.rsqrt(spread / D + EPS_NORM)
    center = jnp.broadcast_to(center, (ROWS, ROWS)).T[:, 0:1]
    scale = jnp.broadcast_to(scale, (ROWS, ROWS)).T[:, 0:1]
    out[...] = ((value - center) * scale * norm2_gain[...]).astype(BF16)

    stage("drain")
    for copy in pending:
        copy.wait_send()
    stage(None)


def shards(*args):
    (
        resid,
        qa_nope,
        qb_nope,
        qa_rope,
        qb_rope,
        latent,
        key_rope,
        lat_gain,
        wa_key,
        wa_val,
        wb_key,
        wb_val,
        gain_a,
        gain_b,
        wa_out,
        wb_out,
        norm1_gain,
        ffn_gate,
        ffn_val,
        conv_gate,
        conv_val,
        ffn_down,
        norm2_gain,
    ) = args
    freq = np.float64(THETA) ** (-np.arange(DR // 2) * 2.0 / DR)
    freq = jnp.asarray(np.broadcast_to(freq[:, None], (DR // 2, ROWS)).astype(np.float32))
    vmem = pl.BlockSpec(memory_space=pltpu.VMEM)
    anywhere = pl.BlockSpec(memory_space=pl.ANY)
    operands = (
        freq,
        resid,
        qa_nope,
        qb_nope,
        qa_rope.T,
        qb_rope.T,
        latent,
        key_rope.T,
        lat_gain[None],
        wa_key,
        wa_val,
        wb_key,
        wb_val,
        gain_a[None],
        gain_b[None],
        wa_out,
        wb_out,
        norm1_gain[None],
        ffn_gate,
        ffn_val,
        conv_gate,
        conv_val,
        ffn_down,
        norm2_gain[None],
    )
    specs = [anywhere] * len(operands)
    small = [x for at, x in enumerate(operands) if at not in (15, 16, 22)]
    dma = pltpu.SemaphoreType.DMA
    return pl.pallas_call(
        kernel,
        out_shape=pltpu.VMEM((ROWS, COLS), BF16),
        in_specs=specs,
        out_specs=vmem,
        scratch_shapes=[
            pltpu.VMEM((4, N, N, 80, 128), BF16),
            pltpu.VMEM((N, N, 32, 2 * UNITS), BF16),
            pltpu.VMEM((3 * ROWS, LAT), BF16),
            pltpu.VMEM((3 * ROWS, DR), BF16),
            pltpu.VMEM((3 * ROWS, LAT), F32),
            pltpu.VMEM((3 * ROWS, 128), F32),
            pltpu.VMEM((3 * ROWS, 128), F32),
            pltpu.VMEM((256, D), BF16),
            pltpu.VMEM((UNITS, D), BF16),
            pltpu.VMEM((N, ROWS, COLS), BF16),
            pltpu.VMEM((4, ROWS, COLS), BF16),
            pltpu.VMEM((4, ROWS, COLS), BF16),
            pltpu.VMEM((N, 8, ROWS), F32),
            pltpu.VMEM((N, ROWS, COLS), BF16),
            pltpu.VMEM((N, HALO, COLS), BF16),
            pltpu.VMEM((HALO + ROWS, D), BF16),
            pltpu.VMEM((ROWS, COLS), BF16),
            pltpu.VMEM((HALO + ROWS, 2 * UNITS), F32),
            pltpu.VMEM((ROWS, UNITS), BF16),
            pltpu.VMEM((N, ROWS, COLS), BF16),
            pltpu.VMEM((4, ROWS, COLS), BF16),
            pltpu.VMEM((4, ROWS, COLS), BF16),
            pltpu.VMEM((N, 8, ROWS), F32),
            dma((3,)),
            dma((7,)),
            dma((8,)),
            dma((8,)),
            dma((8,)),
            dma((14,)),
            dma((16,)),
            dma((8,)),
            dma((8,)),
            dma((8,)),
            dma((8,)),
            dma((8,)),
            dma((8,)),
            dma((28,)),
            dma((32,)),
            dma((8,)),
            dma((8,)),
            dma((8,)),
            dma((8,)),
            dma((8,)),
            dma((8,)),
            dma((8,)),
            dma((8,)),
            dma((8,)),
            dma((8,)),
            dma((8,)),
            dma((8,)),
            dma((4,)),
            dma((4,)),
            dma((4,)),
            dma((4,)),
            dma((len(small),)),
            *[pltpu.VMEM(x.shape, x.dtype) for x in small],
        ],
        compiler_params=pltpu.CompilerParams(
            collective_id=0, has_side_effects=True, vmem_limit_bytes=56 * 1024 * 1024
        ),
        cost_estimate=pl.CostEstimate(flops=8_000_000_000, bytes_accessed=20_000_000, transcendentals=4_000_000),
    )(*operands)


def solution(mesh):
    return jax.shard_map(
        shards,
        mesh=mesh,
        in_specs=(
            P("sp", "tp"),
            P("sp", "tp"),
            P("sp", "tp"),
            P("sp", "tp"),
            P("sp", "tp"),
            P("sp", None),
            P("sp", None),
            P(),
            P(None, "tp"),
            P(None, "tp"),
            P(None, "tp"),
            P(None, "tp"),
            P("tp"),
            P("tp"),
            P("tp", None),
            P("tp", None),
            P(),
            P("sp", "tp"),
            P("sp", "tp"),
            P(None, "tp"),
            P(None, "tp"),
            P("tp", None),
            P("tp"),
        ),
        out_specs=P("sp", "tp"),
        check_vma=False,
    )
```
